1024 devices in a mesh: tp: 128 (over z, y), dp: 8 (over x, core).
Axes of the slice: x: 4, y: 4, z: 32, core: 2. Of those that a mesh axis runs over, the one named last changes fastest.
Arguments:
- stream: bfloat16 [256, 4096], P(None, ('dp', 'tp')), may hold values from -16 to 16
- lengths: int32 [256], P('dp'), may hold values from 1 to 64, 2048 in all
- prior_state: float32 [2, 256, 4096], P(None, 'dp', 'tp'), may hold values from -6 to 6
- prior_window: bfloat16 [2, 256, 3, 4096], P(None, 'dp', None, 'tp'), may hold values from -6 to 6
- norm_gain: float32 [2, 4096], P(None, 'dp'), may hold values from 0.1 to 1.9
- w_branch: bfloat16 [2, 4096, 4096], P(None, 'dp', 'tp'), may hold values from -0.09375 to 0.09375
- w_gate_branch: bfloat16 [2, 4096, 4096], P(None, 'dp', 'tp'), may hold values from -0.09375 to 0.09375
- conv_taps: bfloat16 [2, 4, 4096], P(None, None, 'tp'), may hold values from -3 to 3
- w_in_gate: bfloat16 [2, 256, 4096], P(None, None, 'tp'), may hold values from -0.375 to 0.375
- w_rec_gate: bfloat16 [2, 256, 4096], P(None, None, 'tp'), may hold values from -0.375 to 0.375
- decay_param: float32 [2, 4096], P(None, 'tp'), may hold values from -1 to 4
- w_out: bfloat16 [2, 4096, 4096], P(None, 'tp', 'dp'), may hold values from -0.5 to 0.5
Outputs:
- mixed_out: bfloat16 [256, 4096], P(None, ('dp', 'tp'))
- new_state: float32 [2, 256, 4096], P(None, 'dp', 'tp')
- new_window: bfloat16 [2, 256, 3, 4096], P(None, 'dp', None, 'tp')
The draws below stay inside these ranges and needn't reach their ends.
All inputs are finite; a program needn't handle non-finite values. No bound on the sum of `lengths` on one device may be relied on, other than what follows from the above.
Results may differ from the reference program's by a relative error of at most 0.014.
Values may be sent and summed in bfloat16 or wider, within the bound.
No kernel may reach another device: no remote copies, remote signals or barrier semaphores. Data moves between devices by JAX's collectives and lax.ppermute only.
A program may use at most 32 MiB of HBM per device.

```python
import math
import jax
import jax.numpy as jnp
import numpy as np
from jax import lax

D = 4096
D_RNN = 4096
BLOCK = 256
TAPS = 4
LAYERS = 2
BATCH = 256
N_TP = 128
N_DP = 8


def draw_stream(key, part):
    feature = jnp.arange(D)
    per_device = D // (N_DP * N_TP)
    along_dp = (feature // (D // N_DP)).astype(jnp.float32) / max(N_DP - 1, 1)
    along_tp = (feature // per_device % N_TP).astype(jnp.float32) / max(N_TP - 1, 1)
    rising = jnp.exp(jnp.log(3.0) * (along_dp + along_tp))
    values = jax.random.normal(key, (BATCH, D), jnp.float32) * 0.4 * rising
    return jnp.clip(values, -16.0, 16.0).astype(jnp.bfloat16)


def strengthened(values, stream_key, source, target, shards_of, factor):
    def block_of(axis_at):
        return (jnp.arange(values.shape[axis_at]) // (values.shape[axis_at] // shards_of)).reshape((-1,) + (1,) * (values.ndim - 1 - axis_at))

    near = jax.random.permutation(stream_key, shards_of)[block_of(target)]
    far = (block_of(target) + shards_of // 2) % shards_of
    return jnp.where((block_of(source) == near) | (block_of(source) == far), factor * values, values)


def levels(own_key, dims, split, least, largest):
    def one(axis_at, shards_of):
        draws = jax.random.uniform(jax.random.fold_in(jax.random.fold_in(own_key, 6), axis_at), (shards_of,), jnp.float32, least / len(split), largest / len(split))
        return jnp.repeat(jnp.exp(draws), dims[axis_at] // shards_of).reshape((-1,) + (1,) * (len(dims) - axis_at - 1))

    loudness = one(*split[0])
    for cut in split[1:]:
        loudness = loudness * one(*cut)
    return loudness


def split_up(amount, total, most, lean):
    portions = [(1 << 20) // math.isqrt(standing ** lean) + 1 for standing in range(2, amount + 1)]
    surplus, holding = total - most - (amount - 1), [1] * (amount - 1)
    while surplus > 0:
        candidates = [i for i in range(amount - 1) if holding[i] < most]
        whole, left = sum([portions[i] for i in candidates]), surplus
        for i in candidates:
            addition = min(most - holding[i], max(1, left * portions[i] // whole), surplus)
            holding[i] = holding[i] + addition
            surplus = surplus - addition
    return np.array([most] + holding)


def ragged_sizes(key, count, total, reach, skew):
    if count == 2:
        one = jax.random.randint(key, (), max(1, total - reach), min(reach, total - 1) + 1)
        return jnp.stack([one, total - one])
    sizes = jnp.asarray(split_up(count, total, reach, skew), jnp.int32)
    twos = (count - 1) // 2
    giver, receiver = sizes[1:1 + 2 * twos:2], sizes[2:2 + 2 * twos:2]
    margin = jnp.minimum(giver - 1, reach - receiver)
    moved = jax.random.randint(jax.random.fold_in(key, 1), (twos,), 0, 1 << 20) % (margin + 1)
    sizes = sizes.at[1:1 + 2 * twos:2].set(giver - moved).at[2:2 + 2 * twos:2].set(receiver + moved)
    return sizes[jax.random.permutation(jax.random.fold_in(key, 2), count)]


def gaussian(stream_key, shape, deviation, reach, split=(), held_as=jnp.bfloat16):
    array = deviation * jax.random.normal(stream_key, shape, jnp.float32)
    if split:
        array = array * levels(stream_key, shape, split, -0.22, 0.18)
    return jnp.clip(array, -reach, reach).astype(held_as)


def heavy_noise(stream_key, extent, deviation, most, split, heavy, kind=jnp.bfloat16):
    values = deviation * jax.random.normal(stream_key, extent, jnp.float32)
    if split:
        values = values * levels(stream_key, extent, split, -0.22, 0.18)
    return jnp.clip(strengthened(values, jax.random.fold_in(stream_key, 3), *heavy), -most, most).astype(kind)


def setup_inputs(seed: int = 0) -> dict:
    arg_keys = jax.random.split(jax.random.key(seed), 13)
    stream = draw_stream(jax.random.fold_in(arg_keys[12], 71), 0)
    lengths = ragged_sizes(arg_keys[1], BATCH, 8 * BATCH, 64, 2).astype(jnp.int32)
    prior_state = gaussian(arg_keys[2], (LAYERS, BATCH, D_RNN), 1.0, 6.0, ((1, 8), (2, 128)), jnp.float32)
    prior_window = gaussian(arg_keys[3], (LAYERS, BATCH, TAPS - 1, D_RNN), 1.0, 6.0, ((1, 8), (3, 128)))
    norm_gain = jnp.clip(1.0 + 0.18 * jax.random.normal(arg_keys[4], (LAYERS, D), jnp.float32), 0.1, 1.9)
    w_branch = gaussian(arg_keys[5], (LAYERS, D, D_RNN), D ** -0.5, 0.09375, ((1, 8), (2, 128)))
    w_gate_branch = gaussian(arg_keys[6], (LAYERS, D, D_RNN), D ** -0.5, 0.09375, ((1, 8), (2, 128)))
    conv_taps = gaussian(arg_keys[7], (LAYERS, TAPS, D_RNN), TAPS ** -0.5, 3.0, ((2, 128),))
    w_in_gate = gaussian(arg_keys[8], (LAYERS, BLOCK, D_RNN), BLOCK ** -0.5, 0.375, ((2, 128),))
    w_rec_gate = gaussian(arg_keys[9], (LAYERS, BLOCK, D_RNN), BLOCK ** -0.5, 0.375, ((2, 128),))
    decay_param = jnp.clip(-1.0 + 5.0 * jax.random.uniform(arg_keys[10], (LAYERS, D_RNN), jnp.float32) ** levels(arg_keys[10], (LAYERS, D_RNN), ((1, 128),), -0.2, 0.2), -1.0, 4.0)
    w_out = heavy_noise(arg_keys[11], (LAYERS, D_RNN, D), (D_RNN // 2) ** -0.5, 0.5, ((1, 128), (2, 8)), (1, 2, 128, 5.5))
    return {"stream": stream, "lengths": lengths, "prior_state": prior_state, "prior_window": prior_window, "norm_gain": norm_gain, "w_branch": w_branch, "w_gate_branch": w_gate_branch, "conv_taps": conv_taps, "w_in_gate": w_in_gate, "w_rec_gate": w_rec_gate, "decay_param": decay_param, "w_out": w_out}


epsilon = 1e-06

def block_map(convolved, weight):
    row_count = convolved.shape[0]
    blocks = D_RNN // BLOCK
    inputs = convolved.astype(jnp.float32).reshape(row_count, blocks, BLOCK)
    tables = weight.astype(jnp.float32).reshape(BLOCK, blocks, BLOCK)
    return jnp.einsum('rnk,knc->rnc', inputs, tables).reshape(row_count, D_RNN)

def projected(normed, weight):
    block_width = D // N_DP

    def add_block(running, index):
        offset = (index * block_width).astype(jnp.int32)
        columns = lax.dynamic_slice_in_dim(normed, offset, block_width, 1)
        weight_rows = lax.dynamic_slice_in_dim(weight, offset, block_width, 0)
        partial_sum = jnp.dot(columns, weight_rows, preferred_element_type=jnp.float32).astype(jnp.bfloat16)
        partial_sum = lax.optimization_barrier(partial_sum)
        return (running + partial_sum.astype(jnp.float32), None)
    start_sum = jnp.zeros((normed.shape[0], weight.shape[1]), jnp.float32)
    running, _ = lax.scan(add_block, start_sum, jnp.arange(N_DP, dtype=jnp.int32))
    return running.astype(jnp.bfloat16)

def recurrent_block(stream, lengths, prior_state, prior_window, norm_gain, w_branch, w_gate_branch, conv_taps, w_in_gate, w_rec_gate, decay_param, w_out):
    widened = stream.astype(jnp.float32)
    squares = lax.optimization_barrier(jnp.sum(widened * widened, axis=1, keepdims=True))
    normed = (widened * lax.rsqrt(squares / D + epsilon) * norm_gain).astype(jnp.bfloat16)
    branch = projected(normed, w_branch)
    gate_in = projected(normed, w_gate_branch)
    depth = prior_window.shape[1]
    needed = depth + 1 - jnp.arange(depth, dtype=jnp.int32)
    living = lengths[:, None, None] >= needed[None, :, None]
    history = jnp.where(living, prior_window, jnp.zeros_like(prior_window))
    window = jnp.concatenate([history, branch[:, None, :]], axis=1)
    convolved = lax.optimization_barrier(jnp.sum(window.astype(jnp.float32) * conv_taps.astype(jnp.float32)[None], axis=1)).astype(jnp.bfloat16)
    input_gate = jax.nn.sigmoid(block_map(convolved, w_in_gate))
    recur_gate = jax.nn.sigmoid(block_map(convolved, w_rec_gate))
    log_keep = 8.0 * recur_gate * jax.nn.log_sigmoid(decay_param)
    keeping = jnp.exp(log_keep)
    feeding = jnp.sqrt(-jnp.expm1(2.0 * log_keep))
    earlier = jnp.where(lengths[:, None] >= 2, prior_state, jnp.zeros_like(prior_state))
    state = keeping * earlier + feeding * input_gate * convolved.astype(jnp.float32)
    readout = (state * jax.nn.gelu(gate_in.astype(jnp.float32))).astype(jnp.bfloat16)
    result = (widened + jnp.dot(readout, w_out, preferred_element_type=jnp.float32)).astype(jnp.bfloat16)
    return (result, state, window[:, 1:])

def reference(stream, lengths, prior_state, prior_window, norm_gain, w_branch, w_gate_branch, conv_taps, w_in_gate, w_rec_gate, decay_param, w_out):
    first, state_first, window_first = recurrent_block(stream, lengths, prior_state[0], prior_window[0], norm_gain[0], w_branch[0], w_gate_branch[0], conv_taps[0], w_in_gate[0], w_rec_gate[0], decay_param[0], w_out[0])
    second, state_second, window_second = recurrent_block(first, lengths, prior_state[1], prior_window[1], norm_gain[1], w_branch[1], w_gate_branch[1], conv_taps[1], w_in_gate[1], w_rec_gate[1], decay_param[1], w_out[1])
    return (second, jnp.stack([state_first, state_second]), jnp.stack([window_first, window_second]))
```

```python
import jax
import jax.numpy as jnp
from jax import lax
from jax.sharding import Mesh
from jax.sharding import PartitionSpec as P

D = 4096
BLOCK = 256
TP = ("tp_0", "tp_1")
DP_TP = ("dp", "tp_0", "tp_1")


epsilon = 1e-06


def laid_out(tiles, dim):
    shape = list(tiles.shape[1:])
    shape[dim] *= tiles.shape[0]
    return jnp.moveaxis(tiles, 0, dim).reshape(shape)


def gathered_by_axis(array, axes, turns, dim):
    for k in turns:
        array = copy_for_each(array, axes[k])
    carried = array.shape[: len(turns)]
    rest = array.shape[len(turns) :]
    turned = sorted(range(len(turns)), key=lambda place: turns[len(turns) - 1 - place])
    tiles = array.transpose(*turned, *range(len(turns), array.ndim)).reshape(-1, *rest)
    return laid_out(tiles, dim)


def copy_for_each(array, axis):
    devices = lax.axis_size(axis)
    return lax.all_to_all(
        jnp.broadcast_to(array[None], (devices, *array.shape)), axis, 0, 0, tiled=True
    )


def over_copies(array, axis):
    everything = copy_for_each(array, axis)
    return jnp.sum(everything, axis=0)


def from_partner(block, axis, apart):
    count = lax.axis_size(axis)
    route = []
    for low in range(count):
        high = low | 1 << apart
        if high != low and high < count:
            route += [(low, high), (high, low)]
    return lax.ppermute(block, axis, route)


def in_blocks(array, dim, devices):
    before, after = (array.shape[:dim], array.shape[dim + 1 :])
    return jnp.moveaxis(array.reshape(*before, devices, -1, *after), dim, 0)


def summed_on_arrival(array, axis, dim):
    tiles = in_blocks(array, dim, lax.axis_size(axis))
    arrived = lax.all_to_all(tiles, axis, split_axis=0, concat_axis=0, tiled=True)
    return arrived.astype(jnp.float32).sum(axis=0)


def gather_directly(array, axis, dim):
    tiles = copy_for_each(array, axis)
    return laid_out(tiles, dim)


def to_own_features(terms, stream_local):
    rows, width = terms.shape
    far, near = (lax.axis_size(axis) for axis in TP)
    tiles = terms.astype(jnp.bfloat16).reshape(rows, far, near, -1)
    tiles = summed_on_arrival(tiles, TP[1], 2)[:, :, 0]
    own = summed_on_arrival(tiles.astype(jnp.bfloat16), TP[0], 1)[:, 0]
    return (own + stream_local.astype(jnp.float32)).astype(jnp.bfloat16)


def norm_rows(block_rows, gain_values, squares):
    scaling = lax.rsqrt(squares / D + epsilon)
    return (block_rows.astype(jnp.float32) * scaling * gain_values).astype(jnp.bfloat16)


def normed_input(stream_local, gain_block):
    gathered = gathered_by_axis(stream_local, TP, (0, 1), 1)
    widened = gathered.astype(jnp.float32)
    squares = over_copies(jnp.sum(widened * widened, axis=1, keepdims=True), "dp")
    result = norm_rows(gathered, gain_block, squares)
    return result


def peer_block(convolved):
    col_count = convolved.shape[1]
    group_size = max(BLOCK // col_count, 1)
    device = lax.axis_index(TP)
    grouped = convolved
    for bit_number in range(group_size.bit_length() - 1):
        partner = from_partner(grouped, TP, bit_number)
        is_upper = device // (1 << bit_number) % 2 == 1
        grouped = jnp.where(
            is_upper,
            jnp.concatenate([partner, grouped], axis=1),
            jnp.concatenate([grouped, partner], axis=1),
        )
    return grouped


def block_gates(grouped, weight):
    row_count = grouped.shape[0]
    col_count = weight.shape[1]
    blocks = max(col_count // BLOCK, 1)
    block_cols = min(col_count, BLOCK)
    inputs = grouped.reshape(row_count, blocks, BLOCK)
    tables = weight.reshape(BLOCK, blocks, block_cols)
    mapped = jnp.einsum("rnk,knc->rnc", inputs, tables, preferred_element_type=jnp.float32)
    return mapped.reshape(row_count, col_count)


def recurrent_step(
    normed,
    lengths,
    prior_state,
    prior_window,
    w_branch,
    w_gate_branch,
    conv_taps,
    w_in_gate,
    w_rec_gate,
    decay_param,
    w_out,
    stream_local,
):
    col_count = w_branch.shape[1]
    summed = summed_on_arrival(
        jnp.concatenate(
            [
                jnp.dot(normed, w_branch, preferred_element_type=jnp.float32),
                jnp.dot(normed, w_gate_branch, preferred_element_type=jnp.float32),
            ],
            axis=1,
        ).astype(jnp.bfloat16),
        "dp",
        0,
    )
    branch = summed[:, :col_count].astype(jnp.bfloat16)
    gate_in = summed[:, col_count:].astype(jnp.bfloat16)
    depth = prior_window.shape[1]
    needed = depth + 1 - jnp.arange(depth, dtype=jnp.int32)
    living = lengths[:, None, None] >= needed[None, :, None]
    history = jnp.where(living, prior_window, jnp.zeros_like(prior_window))
    window = jnp.concatenate([history, branch[:, None, :]], axis=1)
    convolved = jnp.sum(
        window.astype(jnp.float32) * conv_taps.astype(jnp.float32)[None], axis=1
    ).astype(jnp.bfloat16)
    grouped = peer_block(convolved)
    input_gate = jax.nn.sigmoid(block_gates(grouped, w_in_gate))
    recur_gate = jax.nn.sigmoid(block_gates(grouped, w_rec_gate))
    log_keep = 8.0 * recur_gate * jax.nn.log_sigmoid(decay_param)
    keeping = jnp.exp(log_keep)
    feeding = jnp.sqrt(-jnp.expm1(2.0 * log_keep))
    earlier = jnp.where(lengths[:, None] >= 2, prior_state, jnp.zeros_like(prior_state))
    state = keeping * earlier + feeding * input_gate * convolved.astype(jnp.float32)
    readout = (state * jax.nn.gelu(gate_in.astype(jnp.float32))).astype(jnp.bfloat16)
    mixed = jnp.dot(gather_directly(readout, "dp", 0), w_out, preferred_element_type=jnp.float32)
    terms = to_own_features(mixed, stream_local)
    return (terms, state, window[:, 1:])


def body(
    stream,
    lengths,
    prior_state,
    prior_window,
    norm_gain,
    w_branch,
    w_gate_branch,
    conv_taps,
    w_in_gate,
    w_rec_gate,
    decay_param,
    w_out,
):
    normed = normed_input(stream, norm_gain[0])
    terms, state_first, window_first = recurrent_step(
        normed,
        lengths,
        prior_state[0],
        prior_window[0],
        w_branch[0],
        w_gate_branch[0],
        conv_taps[0],
        w_in_gate[0],
        w_rec_gate[0],
        decay_param[0],
        w_out[0],
        stream,
    )
    first = terms
    normed = normed_input(first, norm_gain[1])
    terms, state_second, window_second = recurrent_step(
        normed,
        lengths,
        prior_state[1],
        prior_window[1],
        w_branch[1],
        w_gate_branch[1],
        conv_taps[1],
        w_in_gate[1],
        w_rec_gate[1],
        decay_param[1],
        w_out[1],
        first,
    )
    second = terms
    return (
        second,
        jnp.stack([state_first, state_second]),
        jnp.stack([window_first, window_second]),
    )


def solution(mesh):
    torus = Mesh(mesh.devices.reshape(32, 4, mesh.shape["dp"]), ("tp_0", "tp_1", "dp"))
    in_specs = (
        P(None, DP_TP),
        P("dp"),
        P(None, "dp", TP),
        P(None, "dp", None, TP),
        P(None, "dp"),
        P(None, "dp", TP),
        P(None, "dp", TP),
        P(None, None, TP),
        P(None, None, TP),
        P(None, None, TP),
        P(None, TP),
        P(None, TP, "dp"),
    )
    out_specs = (P(None, DP_TP), P(None, "dp", TP), P(None, "dp", None, TP))
    return jax.shard_map(body, mesh=torus, in_specs=in_specs, out_specs=out_specs, check_vma=False)
```

```python
import jax
import jax.numpy as jnp
from jax import lax
from jax.sharding import Mesh
from jax.sharding import PartitionSpec as P

D = 4096
BLOCK = 256
LAYERS = 2
TAPS = 4
AXES = ("zh", "zm", "zl", "y", "x", "core")
Z = ("zh", "zm", "zl")
ZQ = ("zm", "zl")
TP = ("zh", "zm", "zl", "y")
DP = ("x", "core")
PLANE = ("x", "core", "y")
PAIRED = ("zl", "y")
PAIRED_PLANE = ("zl", "y", "x", "core")
bf16 = jnp.bfloat16
f32 = jnp.float32


epsilon = 1e-06


def exchange(tiles, axes):
    return lax.all_to_all(tiles, axes, 0, 0, tiled=True)


def everywhere(array, axes):
    count = lax.axis_size(axes)
    return exchange(jnp.broadcast_to(array[None], (count, *array.shape)), axes)


def contract(a, a_dim, b, b_dim):
    return lax.dot_general(a, b, (((a_dim,), (b_dim,)), ((), ())), preferred_element_type=f32)


def grouped_features(rows_by_feature):
    width = rows_by_feature.shape[1]
    to = jnp.arange(width, dtype=jnp.int32)
    source = (to % 128) // 4 * 16 + to // 128 * 4 + to % 4
    chosen = (jnp.arange(width, dtype=jnp.int32)[:, None] == source[None, :]).astype(bf16)
    return contract(rows_by_feature, 1, chosen, 0).astype(bf16)


def gated_step(layer, branch, gate_in, upper, history, taps, gates, decay, earlier):
    convolved = (
        jnp.sum(history * taps[:3, None], axis=0) + branch.astype(f32) * taps[3]
    ).astype(bf16)
    half = BLOCK // 2
    mapped = [
        contract(convolved[:, :half], 1, gates[kind, 0], 1)
        + contract(convolved[:, half:], 1, gates[kind, 1], 1)
        for kind in range(2)
    ]
    own = jnp.where(upper, convolved[:, half:], convolved[:, :half])
    input_gate = jax.nn.sigmoid(mapped[0])
    recur_gate = jax.nn.sigmoid(mapped[1])
    log_keep = 8.0 * recur_gate * decay
    keeping = jnp.exp(log_keep)
    feeding = jnp.sqrt(-jnp.expm1(2.0 * log_keep))
    state = keeping * earlier + feeding * input_gate * own.astype(f32)
    readout = (state * jax.nn.gelu(gate_in.astype(f32))).astype(bf16)
    own_branch = jnp.where(upper, branch[:, half:], branch[:, :half])
    return state, own_branch, readout


def body(
    stream,
    lengths,
    prior_state,
    prior_window,
    norm_gain,
    w_branch,
    w_gate_branch,
    conv_taps,
    w_in_gate,
    w_rec_gate,
    decay_param,
    w_out,
):
    q = lax.axis_index(ZQ)
    zl = lax.axis_index("zl")
    y = lax.axis_index("y")
    upper = zl == 1

    stream_t = everywhere(stream.T, Z).reshape(128, 256)

    def scaled(weight, layer):
        return (weight[layer].T.astype(f32) * norm_gain[layer]).astype(bf16)

    by_feature = grouped_features(
        jnp.concatenate(
            [
                scaled(w_branch, 0),
                scaled(w_gate_branch, 0),
                scaled(w_branch, 1),
                scaled(w_gate_branch, 1),
                w_out[0],
                w_out[1],
            ],
            axis=0,
        )
    ).reshape(6, 32, 4, 128)
    gate_rows = (
        jnp.stack([w_in_gate, w_rec_gate], axis=1)
        .reshape(LAYERS, 2, 2, 128, 32)
        .transpose(0, 1, 2, 4, 3)
        .reshape(256, 128)
    )
    near = jnp.concatenate(
        [
            by_feature[:2].transpose(2, 0, 1, 3).reshape(4, 64, 128),
            by_feature[5].transpose(1, 0, 2),
            jnp.broadcast_to(gate_rows[None], (4, 256, 128)),
        ],
        axis=1,
    )
    near = exchange(near, "y")
    w_first = near[:, :64].reshape(4, 2, 32, 128).transpose(1, 0, 2, 3).reshape(2, 128, 128)
    w_last = near[:, 64:96].reshape(128, 128)
    gates = (
        near[:, 96:]
        .reshape(4, LAYERS, 2, 2, 32, 128)
        .transpose(1, 2, 3, 0, 4, 5)
        .reshape(LAYERS, 2, 2, 128, 128)
    )

    depth = TAPS - 1
    needed = depth + 1 - jnp.arange(depth, dtype=jnp.int32)
    living = lengths[None, :, None, None] >= needed[None, None, :, None]
    history = jnp.where(living, prior_window, jnp.zeros_like(prior_window))
    earlier = jnp.where(
        lengths[None, :, None] >= 2, prior_state, jnp.zeros_like(prior_state)
    )
    small = jnp.concatenate(
        [
            earlier.reshape(LAYERS, 4, 8, 32).transpose(1, 0, 2, 3).reshape(4, -1),
            history.astype(f32)
            .reshape(LAYERS, 4, 8, depth, 32)
            .transpose(1, 0, 3, 2, 4)
            .reshape(4, -1),
            jnp.broadcast_to(conv_taps.astype(f32).reshape(1, -1), (4, 256)),
            jnp.broadcast_to(jax.nn.log_sigmoid(decay_param).reshape(1, -1), (4, 64)),
            jnp.zeros((4, 64), f32),
        ],
        axis=1,
    ).reshape(1, 4, 19, 128)
    small = exchange(jnp.broadcast_to(small, (2, 4, 19, 128)).reshape(8, 19, 128), PAIRED)
    small = small.reshape(2, 4, -1)

    def own_half(parts):
        return jnp.where(upper, parts[1], parts[0])

    earlier_rows = (
        own_half(small)[:, :512].reshape(4, LAYERS, 8, 32).transpose(1, 2, 0, 3)
    ).reshape(LAYERS, 8, 128)
    history_rows = (
        small[:, :, 512:2048]
        .reshape(8, LAYERS, depth, 8, 32)
        .transpose(1, 2, 3, 0, 4)
        .reshape(LAYERS, depth, 8, 256)
    )
    taps = (
        small[:, :, 2048:2304]
        .reshape(8, LAYERS, TAPS, 32)
        .transpose(1, 2, 0, 3)
        .reshape(LAYERS, TAPS, 256)
    )
    decay = (
        own_half(small)[:, 2304:2368].reshape(4, LAYERS, 32).transpose(1, 0, 2)
    ).reshape(LAYERS, 1, 128)

    w_mid = everywhere(by_feature[4].reshape(32, 512), PLANE)
    w_mid = (
        w_mid.reshape(8, 4, 32, 4, 128).transpose(1, 2, 3, 0, 4).reshape(128, 4096)
    )
    w_second = exchange(by_feature[2:4].transpose(2, 0, 1, 3).reshape(4, 64, 128), ZQ)
    w_second = everywhere(w_second, PLANE)
    w_second = (
        w_second.reshape(8, 4, 4, 2, 32, 128).transpose(2, 3, 1, 4, 0, 5).reshape(1024, 1024)
    )

    stream_rows = stream_t.T.reshape(8, 4, 8, 128).transpose(1, 0, 2, 3)
    products = [
        contract(stream_t, 0, w_first[kind], 1)
        .astype(bf16)
        .reshape(8, 4, 8, 128)
        .transpose(1, 0, 2, 3)
        for kind in range(2)
    ]
    sent = jnp.stack(
        [
            jnp.stack([products[0], jnp.where(upper, stream_rows, products[1])], axis=2),
            jnp.stack([products[0], jnp.where(upper, products[1], stream_rows)], axis=2),
        ]
    )
    came = exchange(sent.reshape(64, 16, 128), PAIRED_PLANE).reshape(2, 32, 2, 8, 128)
    branch = came[:, :, 0].astype(f32).sum(axis=1)
    branch = jnp.concatenate([branch[0], branch[1]], axis=1)
    rows = jnp.where(upper, came[0, :, 1], came[1, :, 1])
    gate_in = jnp.where(upper, came[1, :, 1], came[0, :, 1]).astype(f32).sum(axis=0)
    widened = rows.astype(f32)
    squares = jnp.sum(jnp.sum(widened * widened, axis=0), axis=1, keepdims=True)
    scaling = lax.rsqrt(squares / D + epsilon)
    state_first, branch_first, readout = gated_step(
        0,
        (branch * scaling).astype(bf16),
        (gate_in * scaling).astype(bf16),
        upper,
        history_rows[0],
        taps[0],
        gates[0],
        decay[0],
        earlier_rows[0],
    )
    residual = lax.dynamic_index_in_dim(rows.reshape(4, 8, 8, 128), q, 0, keepdims=False)
    mixed = contract(readout, 1, w_mid, 0).astype(bf16)
    mixed = exchange(mixed.reshape(8, 4, 8, 128).transpose(1, 2, 0, 3), ZQ)
    mixed = mixed.astype(f32).sum(axis=0).astype(bf16)
    mixed = everywhere(mixed, "zh").astype(f32).sum(axis=0)
    first = (mixed + residual.astype(f32)).astype(bf16)

    first_rows = first.transpose(1, 0, 2).reshape(8, 1024)
    widened = first_rows.astype(f32)
    squares = jnp.sum(widened * widened, axis=1, keepdims=True)
    coarse = lax.reduce_precision(squares, 8, 7)
    lane = lax.broadcasted_iota(jnp.int32, (8, 128), 1)
    squares = jnp.where(lane < 64, coarse, squares - coarse).astype(bf16)
    products = contract(first_rows, 1, w_second, 1).astype(bf16)
    products = products.reshape(8, 2, 2, 2, 128)
    sent = jnp.stack(
        [
            jnp.stack(
                [products[:, zm, 0, 0], products[:, zm, 1, 0], products[:, zm, low, 1], squares]
            )
            for zm in range(2)
            for low in range(2)
        ]
    )
    came = exchange(sent, ZQ).astype(f32).sum(axis=0)
    branch = jnp.concatenate([came[0], came[1]], axis=1)
    squares = came[3, :, :1] + came[3, :, 64:65]
    scaling = lax.rsqrt(squares / D + epsilon)
    state_second, branch_second, readout = gated_step(
        1,
        (branch * scaling).astype(bf16),
        (came[2] * scaling).astype(bf16),
        upper,
        history_rows[1],
        taps[1],
        gates[1],
        decay[1],
        earlier_rows[1],
    )
    sent = jnp.stack(
        [
            jnp.broadcast_to(readout[None, None], (8, 4, 8, 128)),
            jnp.broadcast_to(first[:, None], (8, 4, 8, 128)),
        ],
        axis=2,
    )
    came = exchange(sent.reshape(32, 16, 128), PLANE).reshape(32, 2, 8, 128)
    came = jnp.concatenate(
        [came[:, 0].reshape(256, 128), came[:, 1].reshape(256, 128)], axis=1
    )
    adds = (q == y) & (lax.axis_index("zh") == 0)
    index = lax.broadcasted_iota(jnp.int32, (128, 128), 0)
    same = index == lax.broadcasted_iota(jnp.int32, (128, 128), 1)
    same = jnp.where(same & adds, 1.0, 0.0).astype(bf16)
    mixed = contract(jnp.concatenate([w_last, same], axis=0), 0, came, 1).astype(bf16)
    second = exchange(mixed.reshape(32, 4, 256), Z).astype(f32).sum(axis=0).astype(bf16)

    kept = jnp.stack(
        [state_first, state_second, branch_first.astype(f32), branch_second.astype(f32)]
    )
    kept = exchange(kept.reshape(4, 8, 4, 32).transpose(2, 0, 1, 3).reshape(4, 8, 128), "y")
    kept = kept.reshape(4, 4, 8, 32).transpose(1, 0, 2, 3).reshape(2, LAYERS, 32, 32)
    window = jnp.concatenate([history[:, :, 1:], kept[1].astype(bf16)[:, :, None]], axis=2)
    return second.T, kept[0], window


def solution(mesh):
    torus = Mesh(mesh.devices.reshape(8, 2, 2, 4, 4, 2), AXES)
    in_specs = (
        P(None, DP + TP),
        P(DP),
        P(None, DP, TP),
        P(None, DP, None, TP),
        P(None, DP),
        P(None, DP, TP),
        P(None, DP, TP),
        P(None, None, TP),
        P(None, None, TP),
        P(None, None, TP),
        P(None, TP),
        P(None, TP, DP),
    )
    out_specs = (P(None, DP + TP), P(None, DP, TP), P(None, DP, None, TP))
    return jax.shard_map(body, mesh=torus, in_specs=in_specs, out_specs=out_specs, check_vma=False)
```

```python
import jax
import jax.numpy as jnp
from jax import lax
from jax.sharding import Mesh
from jax.sharding import PartitionSpec as P

D = 4096
BLOCK = 256
LAYERS = 2
TAPS = 4
AXES = ("zh", "zm", "zl", "y", "x", "core")
Z = ("zh", "zm", "zl")
ZQ = ("zm", "zl")
TP = ("zh", "zm", "zl", "y")
DP = ("x", "core")
PLANE = ("x", "core", "y")
PAIRED_PLANE = ("zl", "y", "x", "core")
bf16 = jnp.bfloat16
f32 = jnp.float32


epsilon = 1e-06


def exchange(tiles, axes):
    return lax.all_to_all(tiles, axes, 0, 0, tiled=True)


def everywhere(array, axes):
    count = lax.axis_size(axes)
    return exchange(jnp.broadcast_to(array[None], (count, *array.shape)), axes)


def passed(piece, axis, step):
    count = lax.axis_size(axis)
    return lax.ppermute(piece, axis, [(at, (at + step) % count) for at in range(count)])


def traded(tiles, axis):
    count = lax.axis_size(axis)
    here = lax.axis_index(axis)
    pieces = []
    for step in range(count):
        piece = lax.dynamic_index_in_dim(tiles, (here + step) % count, 0, keepdims=False)
        pieces.append(passed(piece, axis, step) if step else piece)
    return pieces


def collected(piece, axis):
    return [piece] + [passed(piece, axis, k) for k in range(1, lax.axis_size(axis))]


def in_order(pieces, axis):
    backward = jnp.stack(pieces[::-1] + pieces[::-1])
    count = len(pieces)
    return lax.dynamic_slice_in_dim(backward, count - 1 - lax.axis_index(axis), count, 0)


def relative(tiles):
    parts = tiles.reshape(4, 2, *tiles.shape[1:])
    parts = jnp.concatenate([parts, parts])[::-1]
    parts = lax.dynamic_slice_in_dim(parts, 3 - lax.axis_index("x"), 4, 0)
    return jnp.where(lax.axis_index("core") == 1, parts[:, ::-1], parts).reshape(tiles.shape)


def parts_of(value):
    coarse = lax.reduce_precision(value, 8, 7)
    rest = value - coarse
    middle = lax.reduce_precision(rest, 8, 7)
    return [coarse.astype(bf16), middle.astype(bf16), (rest - middle).astype(bf16)]


def whole_of(coarse, middle, fine):
    return coarse.astype(f32) + (middle.astype(f32) + fine.astype(f32))


def over_dp(piece):
    pieces = jnp.stack(collected(piece, "x"))
    return [pieces, passed(pieces, "core", 1)]


def contract(a, a_dim, b, b_dim):
    return lax.dot_general(a, b, (((a_dim,), (b_dim,)), ((), ())), preferred_element_type=f32)


def grouped_features(rows_by_feature):
    width = rows_by_feature.shape[1]
    to = jnp.arange(width, dtype=jnp.int32)
    source = (to % 128) // 4 * 16 + to // 128 * 4 + to % 4
    chosen = (jnp.arange(width, dtype=jnp.int32)[:, None] == source[None, :]).astype(bf16)
    return contract(rows_by_feature, 1, chosen, 0).astype(bf16)


def gated_step(layer, branch, gate_in, upper, history, taps, gates, decay, earlier):
    convolved = (
        jnp.sum(history * taps[:3, None], axis=0) + branch.astype(f32) * taps[3]
    ).astype(bf16)
    half = BLOCK // 2
    mapped = [
        contract(convolved[:, :half], 1, gates[kind, 0], 1)
        + contract(convolved[:, half:], 1, gates[kind, 1], 1)
        for kind in range(2)
    ]
    own = jnp.where(upper, convolved[:, half:], convolved[:, :half])
    input_gate = jax.nn.sigmoid(mapped[0])
    recur_gate = jax.nn.sigmoid(mapped[1])
    log_keep = 8.0 * recur_gate * decay
    keeping = jnp.exp(log_keep)
    feeding = jnp.sqrt(-jnp.expm1(2.0 * log_keep))
    state = keeping * earlier + feeding * input_gate * own.astype(f32)
    readout = (state * jax.nn.gelu(gate_in.astype(f32))).astype(bf16)
    own_branch = jnp.where(upper, branch[:, half:], branch[:, :half])
    return state, own_branch, readout


def body(
    stream,
    lengths,
    prior_state,
    prior_window,
    norm_gain,
    w_branch,
    w_gate_branch,
    conv_taps,
    w_in_gate,
    w_rec_gate,
    decay_param,
    w_out,
):
    q = lax.axis_index(ZQ)
    zl = lax.axis_index("zl")
    y = lax.axis_index("y")
    upper = zl == 1

    stream_t = everywhere(stream.T, Z).reshape(128, 256)

    def scaled(weight, layer):
        return (weight[layer].T.astype(f32) * norm_gain[layer]).astype(bf16)

    by_feature = grouped_features(
        jnp.concatenate(
            [
                scaled(w_branch, 0),
                scaled(w_gate_branch, 0),
                scaled(w_branch, 1),
                scaled(w_gate_branch, 1),
                w_out[0],
                w_out[1],
            ],
            axis=0,
        )
    ).reshape(6, 32, 4, 128)
    gate_rows = (
        jnp.stack([w_in_gate, w_rec_gate], axis=1)
        .reshape(LAYERS, 2, 2, 128, 32)
        .transpose(0, 1, 2, 4, 3)
        .reshape(256, 128)
    )
    depth = TAPS - 1
    needed = depth + 1 - jnp.arange(depth, dtype=jnp.int32)
    living = lengths[None, :, None, None] >= needed[None, None, :, None]
    history = jnp.where(living, prior_window, jnp.zeros_like(prior_window))
    earlier = jnp.where(
        lengths[None, :, None] >= 2, prior_state, jnp.zeros_like(prior_state)
    )
    earlier = earlier.reshape(LAYERS, 4, 8, 32).transpose(1, 0, 2, 3).reshape(4, -1)
    decay = jnp.broadcast_to(jax.nn.log_sigmoid(decay_param).reshape(1, -1), (4, 64))
    small = jnp.concatenate(
        parts_of(earlier)
        + parts_of(decay)
        + [
            history.reshape(LAYERS, 4, 8, depth, 32).transpose(1, 0, 3, 2, 4).reshape(4, -1),
            jnp.broadcast_to(conv_taps.reshape(1, -1), (4, 256)),
            jnp.zeros((4, 64), bf16),
        ],
        axis=1,
    ).reshape(4, 28, 128)
    near = jnp.concatenate(
        [
            by_feature[:2].transpose(2, 0, 1, 3).reshape(4, 64, 128),
            by_feature[5].transpose(1, 0, 2),
            jnp.broadcast_to(gate_rows[None], (4, 256, 128)),
            jnp.broadcast_to(by_feature[4].transpose(1, 0, 2).reshape(1, 128, 128), (4, 128, 128)),
            small,
        ],
        axis=1,
    )
    near = in_order(traded(near, "y"), "y")
    w_first = near[:, :64].reshape(4, 2, 32, 128).transpose(1, 0, 2, 3).reshape(2, 128, 128)
    w_last = near[:, 64:96].reshape(128, 128)
    gates = (
        near[:, 96:352]
        .reshape(4, LAYERS, 2, 2, 32, 128)
        .transpose(1, 2, 3, 0, 4, 5)
        .reshape(LAYERS, 2, 2, 128, 128)
    )
    w_mid = near[:, 352:480].reshape(4, 4, 32, 128).transpose(1, 0, 2, 3).reshape(4, 128, 128)
    small = near[:, 480:].reshape(4, 3584)

    earlier_rows = (
        whole_of(small[:, :512], small[:, 512:1024], small[:, 1024:1536])
        .reshape(4, LAYERS, 8, 32)
        .transpose(1, 2, 0, 3)
        .reshape(LAYERS, 8, 128)
    )
    decay = (
        whole_of(small[:, 1536:1600], small[:, 1600:1664], small[:, 1664:1728])
        .reshape(4, LAYERS, 32)
        .transpose(1, 0, 2)
        .reshape(LAYERS, 1, 128)
    )
    windows = jnp.concatenate(
        [
            small[:, 1728:3264].reshape(4, 48, 32).transpose(1, 0, 2).reshape(48, 128),
            small[:, 3264:3520].reshape(4, 8, 32).transpose(1, 0, 2).reshape(8, 128),
        ],
        axis=0,
    )
    partner = passed(windows, "zl", 1)
    windows = jnp.concatenate(
        [jnp.where(upper, partner, windows), jnp.where(upper, windows, partner)], axis=1
    ).astype(f32)
    history_rows = windows[:48].reshape(LAYERS, depth, 8, 256)
    taps = windows[48:].reshape(LAYERS, TAPS, 256)

    w_mid = over_dp(w_mid)
    w_second = by_feature[2:4].transpose(2, 0, 1, 3).reshape(4, 64, 128)
    w_second = in_order(traded(w_second, ZQ), ZQ).reshape(256, 128)
    w_second = in_order(collected(w_second, "y"), "y")
    w_second = (
        w_second.reshape(4, 4, 2, 32, 128).transpose(1, 2, 0, 3, 4).reshape(1024, 128)
    )
    w_second = over_dp(w_second)

    stream_rows = stream_t.T.reshape(8, 4, 8, 128).transpose(1, 0, 2, 3)
    products = [
        contract(stream_t, 0, w_first[kind], 1)
        .astype(bf16)
        .reshape(8, 4, 8, 128)
        .transpose(1, 0, 2, 3)
        for kind in range(2)
    ]
    sent = jnp.stack(
        [
            jnp.stack([products[0], jnp.where(upper, stream_rows, products[1])], axis=2),
            jnp.stack([products[0], jnp.where(upper, products[1], stream_rows)], axis=2),
        ]
    )
    came = exchange(sent.reshape(64, 16, 128), PAIRED_PLANE).reshape(2, 32, 2, 8, 128)
    branch = came[:, :, 0].astype(f32).sum(axis=1)
    branch = jnp.concatenate([branch[0], branch[1]], axis=1)
    rows = jnp.where(upper, came[0, :, 1], came[1, :, 1])
    gate_in = jnp.where(upper, came[1, :, 1], came[0, :, 1]).astype(f32).sum(axis=0)
    widened = rows.astype(f32)
    squares = jnp.sum(jnp.sum(widened * widened, axis=0), axis=1, keepdims=True)
    scaling = lax.rsqrt(squares / D + epsilon)
    state_first, branch_first, readout = gated_step(
        0,
        (branch * scaling).astype(bf16),
        (gate_in * scaling).astype(bf16),
        upper,
        history_rows[0],
        taps[0],
        gates[0],
        decay[0],
        earlier_rows[0],
    )
    residual = lax.dynamic_index_in_dim(rows.reshape(4, 8, 8, 128), q, 0, keepdims=False)
    residual = relative(residual)
    mixed = jnp.stack(
        [
            jnp.stack(
                [
                    jnp.stack([contract(readout, 1, w_mid[core][x, part], 0) for core in range(2)])
                    for x in range(4)
                ]
            )
            for part in range(4)
        ]
    ).astype(bf16)
    mixed = exchange(mixed.reshape(4, 8, 8, 128), ZQ)
    mixed = mixed.astype(f32).sum(axis=0).astype(bf16)
    mixed = everywhere(mixed, "zh").astype(f32).sum(axis=0)
    first = (mixed + residual.astype(f32)).astype(bf16)

    widened = first.astype(f32)
    squares = jnp.sum(jnp.sum(widened * widened, axis=0), axis=1, keepdims=True)
    coarse = lax.reduce_precision(squares, 8, 7)
    lane = lax.broadcasted_iota(jnp.int32, (8, 128), 1)
    squares = jnp.where(lane < 64, coarse, squares - coarse).astype(bf16)
    products = sum(
        contract(first[2 * x + core], 1, w_second[core][x], 1)
        for core in range(2)
        for x in range(4)
    ).astype(bf16)
    products = products.reshape(8, 2, 2, 2, 128)
    sent = jnp.stack(
        [
            jnp.stack(
                [products[:, zm, 0, 0], products[:, zm, 1, 0], products[:, zm, low, 1], squares]
            )
            for zm in range(2)
            for low in range(2)
        ]
    )
    came = exchange(sent, ZQ).astype(f32).sum(axis=0)
    branch = jnp.concatenate([came[0], came[1]], axis=1)
    squares = came[3, :, :1] + came[3, :, 64:65]
    scaling = lax.rsqrt(squares / D + epsilon)
    state_second, branch_second, readout = gated_step(
        1,
        (branch * scaling).astype(bf16),
        (came[2] * scaling).astype(bf16),
        upper,
        history_rows[1],
        taps[1],
        gates[1],
        decay[1],
        earlier_rows[1],
    )
    sent = jnp.stack(
        [
            jnp.broadcast_to(readout[None, None], (8, 4, 8, 128)),
            jnp.broadcast_to(relative(first)[:, None], (8, 4, 8, 128)),
        ],
        axis=2,
    )
    came = exchange(sent.reshape(32, 16, 128), PLANE).reshape(32, 2, 8, 128)
    came = jnp.concatenate(
        [came[:, 0].reshape(256, 128), came[:, 1].reshape(256, 128)], axis=1
    )
    adds = (q == y) & (lax.axis_index("zh") == 0)
    index = lax.broadcasted_iota(jnp.int32, (128, 128), 0)
    same = index == lax.broadcasted_iota(jnp.int32, (128, 128), 1)
    same = jnp.where(same & adds, 1.0, 0.0).astype(bf16)
    mixed = contract(jnp.concatenate([w_last, same], axis=0), 0, came, 1).astype(bf16)
    second = exchange(mixed.reshape(32, 4, 256), Z).astype(f32).sum(axis=0).astype(bf16)

    kept = jnp.stack(
        [state_first, state_second, branch_first.astype(f32), branch_second.astype(f32)]
    )
    kept = kept.reshape(4, 8, 4, 32).transpose(2, 0, 1, 3).reshape(4, 8, 128)
    kept = in_order(traded(kept, "y"), "y")
    kept = kept.reshape(4, 4, 8, 32).transpose(1, 0, 2, 3).reshape(2, LAYERS, 32, 32)
    window = jnp.concatenate([history[:, :, 1:], kept[1].astype(bf16)[:, :, None]], axis=2)
    return second.T, kept[0], window


def solution(mesh):
    torus = Mesh(mesh.devices.reshape(8, 2, 2, 4, 4, 2), AXES)
    in_specs = (
        P(None, DP + TP),
        P(DP),
        P(None, DP, TP),
        P(None, DP, None, TP),
        P(None, DP),
        P(None, DP, TP),
        P(None, DP, TP),
        P(None, None, TP),
        P(None, None, TP),
        P(None, None, TP),
        P(None, TP),
        P(None, TP, DP),
    )
    out_specs = (P(None, DP + TP), P(None, DP, TP), P(None, DP, None, TP))
    return jax.shard_map(body, mesh=torus, in_specs=in_specs, out_specs=out_specs, check_vma=False)
```

```python
import jax
import jax.numpy as jnp
from jax import lax
from jax.sharding import Mesh
from jax.sharding import PartitionSpec as P


D = 4096
BLOCK = 256
LAYERS = 2
TAPS = 4
AXES = ("zh", "zm", "zl", "y", "x", "core")
Z = ("zh", "zm", "zl")
ZQ = ("zm", "zl")
TP = ("zh", "zm", "zl", "y")
DP = ("x", "core")
PLANE = ("x", "core", "y")
PAIRED_PLANE = ("zl", "y", "x", "core")
bf16 = jnp.bfloat16
f32 = jnp.float32


epsilon = 1e-06


def exchange(tiles, axes):
    return lax.all_to_all(tiles, axes, 0, 0, tiled=True)


def everywhere(array, axes):
    count = lax.axis_size(axes)
    return exchange(jnp.broadcast_to(array[None], (count, *array.shape)), axes)


def passed(piece, axis, step):
    count = lax.axis_size(axis)
    return lax.ppermute(piece, axis, [(at, (at + step) % count) for at in range(count)])


def traded(tiles, axis):
    count = lax.axis_size(axis)
    here = lax.axis_index(axis)
    pieces = []
    for step in range(count):
        piece = lax.dynamic_index_in_dim(tiles, (here + step) % count, 0, keepdims=False)
        pieces.append(passed(piece, axis, step) if step else piece)
    return pieces


def in_order(pieces, axis):
    backward = jnp.stack(pieces[::-1] + pieces[::-1])
    count = len(pieces)
    return lax.dynamic_slice_in_dim(backward, count - 1 - lax.axis_index(axis), count, 0)


def parts_of(value):
    coarse = lax.reduce_precision(value, 8, 7)
    rest = value - coarse
    middle = lax.reduce_precision(rest, 8, 7)
    return [coarse.astype(bf16), middle.astype(bf16), (rest - middle).astype(bf16)]


def whole_of(coarse, middle, fine):
    return coarse.astype(f32) + (middle.astype(f32) + fine.astype(f32))


def contract(a, a_dim, b, b_dim):
    return lax.dot_general(a, b, (((a_dim,), (b_dim,)), ((), ())), preferred_element_type=f32)


def grouped_features(rows_by_feature):
    width = rows_by_feature.shape[1]
    to = jnp.arange(width, dtype=jnp.int32)
    source = (to % 128) // 4 * 16 + to // 128 * 4 + to % 4
    chosen = (jnp.arange(width, dtype=jnp.int32)[:, None] == source[None, :]).astype(bf16)
    return contract(rows_by_feature, 1, chosen, 0).astype(bf16)


def gated_step(branch, gate_in, upper, history, taps, gates, decay, earlier):
    convolved = (
        jnp.sum(history * taps[:3, None], axis=0) + branch.astype(f32) * taps[3]
    ).astype(bf16)
    half = BLOCK // 2
    mapped = [
        contract(convolved[:, :half], 1, gates[kind, 0], 1)
        + contract(convolved[:, half:], 1, gates[kind, 1], 1)
        for kind in range(2)
    ]
    own = jnp.where(upper, convolved[:, half:], convolved[:, :half])
    input_gate = jax.nn.sigmoid(mapped[0])
    recur_gate = jax.nn.sigmoid(mapped[1])
    log_keep = 8.0 * recur_gate * decay
    keeping = jnp.exp(log_keep)
    feeding = jnp.sqrt(-jnp.expm1(2.0 * log_keep))
    state = keeping * earlier + feeding * input_gate * own.astype(f32)
    readout = (state * jax.nn.gelu(gate_in.astype(f32))).astype(bf16)
    own_branch = jnp.where(upper, branch[:, half:], branch[:, :half])
    return state, own_branch, readout


def both_blocks(
    stream,
    lengths,
    prior_state,
    prior_window,
    norm_gain,
    w_branch,
    w_gate_branch,
    conv_taps,
    w_in_gate,
    w_rec_gate,
    decay_param,
    w_out,
):
    zl = lax.axis_index("zl")
    upper = zl == 1

    stream_t = everywhere(stream.T, Z).reshape(128, 256)

    def scaled(weight, layer):
        return (weight[layer].T.astype(f32) * norm_gain[layer]).astype(bf16)

    by_feature = grouped_features(
        jnp.concatenate(
            [
                scaled(w_branch, 0),
                scaled(w_gate_branch, 0),
                scaled(w_branch, 1),
                scaled(w_gate_branch, 1),
                w_out[0],
                w_out[1],
            ],
            axis=0,
        )
    ).reshape(6, 32, 4, 128)
    gate_rows = (
        jnp.stack([w_in_gate, w_rec_gate], axis=1)
        .reshape(LAYERS, 2, 2, 128, 32)
        .transpose(0, 1, 2, 4, 3)
        .reshape(256, 128)
    )
    depth = TAPS - 1
    needed = depth + 1 - jnp.arange(depth, dtype=jnp.int32)
    living = lengths[None, :, None, None] >= needed[None, None, :, None]
    history = jnp.where(living, prior_window, jnp.zeros_like(prior_window))
    earlier = jnp.where(
        lengths[None, :, None] >= 2, prior_state, jnp.zeros_like(prior_state)
    )
    earlier = earlier.reshape(LAYERS, 4, 8, 32).transpose(1, 0, 2, 3).reshape(4, -1)
    decay = jnp.broadcast_to(jax.nn.log_sigmoid(decay_param).reshape(1, -1), (4, 64))
    small = jnp.concatenate(
        parts_of(earlier)
        + parts_of(decay)
        + [
            history.reshape(LAYERS, 4, 8, depth, 32).transpose(1, 0, 3, 2, 4).reshape(4, -1),
            jnp.broadcast_to(conv_taps.reshape(1, -1), (4, 256)),
            jnp.zeros((4, 64), bf16),
        ],
        axis=1,
    ).reshape(4, 28, 128)
    near = jnp.concatenate(
        [
            by_feature[:2].transpose(2, 0, 1, 3).reshape(4, 64, 128),
            by_feature[5].transpose(1, 0, 2),
            jnp.broadcast_to(gate_rows[None], (4, 256, 128)),
            jnp.broadcast_to(
                by_feature[2:5].transpose(2, 0, 1, 3).reshape(1, 384, 128), (4, 384, 128)
            ),
            small,
        ],
        axis=1,
    )
    near = in_order(traded(near, "y"), "y")
    w_first = near[:, :64].reshape(4, 2, 32, 128).transpose(1, 0, 2, 3).reshape(2, 128, 128)
    w_last = near[:, 64:96].reshape(128, 128)
    gates = (
        near[:, 96:352]
        .reshape(4, LAYERS, 2, 2, 32, 128)
        .transpose(1, 2, 3, 0, 4, 5)
        .reshape(LAYERS, 2, 2, 128, 128)
    )
    middle = (
        near[:, 352:736].reshape(4, 4, 3, 32, 128).transpose(1, 2, 0, 3, 4).reshape(4, 384, 128)
    )
    small = near[:, 736:].reshape(4, 3584)
    earlier_rows = (
        whole_of(small[:, :512], small[:, 512:1024], small[:, 1024:1536])
        .reshape(4, LAYERS, 8, 32)
        .transpose(1, 2, 0, 3)
        .reshape(LAYERS, 8, 128)
    )
    decay = (
        whole_of(small[:, 1536:1600], small[:, 1600:1664], small[:, 1664:1728])
        .reshape(4, LAYERS, 32)
        .transpose(1, 0, 2)
        .reshape(LAYERS, 1, 128)
    )
    windows = jnp.concatenate(
        [
            small[:, 1728:3264].reshape(4, 48, 32).transpose(1, 0, 2).reshape(48, 128),
            small[:, 3264:3520].reshape(4, 8, 32).transpose(1, 0, 2).reshape(8, 128),
        ],
        axis=0,
    )
    partner = passed(windows, "zl", 1)
    windows = jnp.concatenate(
        [jnp.where(upper, partner, windows), jnp.where(upper, windows, partner)], axis=1
    ).astype(f32)
    history_rows = windows[:48].reshape(LAYERS, depth, 8, 256)
    taps = windows[48:].reshape(LAYERS, TAPS, 256)

    middle = in_order(traded(middle, ZQ), ZQ)
    w_second = middle[:, :256].reshape(1024, 128)
    w_mid = middle[:, 256:].reshape(512, 128)

    stream_rows = stream_t.T.reshape(8, 4, 8, 128).transpose(1, 0, 2, 3)
    products = [
        contract(stream_t, 0, w_first[kind], 1)
        .astype(bf16)
        .reshape(8, 4, 8, 128)
        .transpose(1, 0, 2, 3)
        for kind in range(2)
    ]
    sent = jnp.stack(
        [
            jnp.stack([products[0], jnp.where(upper, stream_rows, products[1])], axis=2),
            jnp.stack([products[0], jnp.where(upper, products[1], stream_rows)], axis=2),
        ]
    )
    came = exchange(sent.reshape(64, 16, 128), PAIRED_PLANE).reshape(2, 32, 2, 8, 128)
    branch = came[:, :, 0].astype(f32).sum(axis=1)
    branch = jnp.concatenate([branch[0], branch[1]], axis=1)
    rows = jnp.where(upper, came[0, :, 1], came[1, :, 1])
    gate_in = jnp.where(upper, came[1, :, 1], came[0, :, 1]).astype(f32).sum(axis=0)
    widened = rows.astype(f32)
    squares = jnp.sum(jnp.sum(widened * widened, axis=0), axis=1, keepdims=True)
    scaling = lax.rsqrt(squares / D + epsilon)
    state_first, branch_first, readout = gated_step(
        (branch * scaling).astype(bf16),
        (gate_in * scaling).astype(bf16),
        upper,
        history_rows[0],
        taps[0],
        gates[0],
        decay[0],
        earlier_rows[0],
    )
    sent = jnp.stack(
        [jnp.broadcast_to(readout[None], (32, 8, 128)), rows], axis=1
    )
    came = exchange(sent.reshape(32, 16, 128), ZQ + DP).reshape(4, 8, 2, 8, 128)
    residual = came[0, :, 1].reshape(64, 128).astype(f32)
    came = came[:, :, 0].reshape(4, 64, 128)
    came = jnp.concatenate([came[at] for at in range(4)], axis=1)
    mixed = contract(came, 1, w_mid, 0).astype(bf16)
    mixed = everywhere(mixed, "zh").astype(f32).sum(axis=0)
    first = (mixed + residual).astype(bf16)

    products = contract(first, 1, w_second, 1).astype(bf16)
    products = [products[:, 128 * at : 128 * (at + 1)].reshape(8, 8, 128) for at in range(8)]
    own_rows = first.reshape(8, 8, 128)
    sent = jnp.stack(
        [
            jnp.stack(
                [
                    products[4 * zm],
                    products[4 * zm + 2],
                    products[4 * zm + 2 * low + 1],
                    own_rows,
                ],
                axis=1,
            )
            for zm in range(2)
            for low in range(2)
        ]
    )
    came = exchange(sent.reshape(32, 32, 128), ZQ + DP).reshape(32, 4, 8, 128)
    rows = came[:, 3]
    came = came[:, :3].astype(f32).sum(axis=0)
    widened = rows.astype(f32)
    squares = jnp.sum(jnp.sum(widened * widened, axis=0), axis=1, keepdims=True)
    branch = jnp.concatenate([came[0], came[1]], axis=1)
    scaling = lax.rsqrt(squares / D + epsilon)
    state_second, branch_second, readout = gated_step(
        (branch * scaling).astype(bf16),
        (came[2] * scaling).astype(bf16),
        upper,
        history_rows[1],
        taps[1],
        gates[1],
        decay[1],
        earlier_rows[1],
    )
    sent = jnp.stack(
        [
            jnp.broadcast_to(readout[None], (32, 8, 128)),
            rows.reshape(4, 8, 8, 128).transpose(1, 0, 2, 3).reshape(32, 8, 128),
        ],
        axis=1,
    )
    came = exchange(sent.reshape(32, 16, 128), PLANE).reshape(32, 2, 8, 128)
    mixed = contract(w_last, 0, came[:, 0].reshape(256, 128), 1).astype(bf16)
    own = lax.broadcasted_iota(jnp.int32, (4, 128), 0) + 4 * lax.axis_index(Z)
    own = (own == lax.broadcasted_iota(jnp.int32, (4, 128), 1)).astype(bf16)
    residual = contract(own, 1, came[:, 1].reshape(256, 128), 1)
    second = exchange(mixed.reshape(32, 4, 256), Z).astype(f32).sum(axis=0)
    second = (second + residual).astype(bf16)

    kept = jnp.stack(
        [state_first, state_second, branch_first.astype(f32), branch_second.astype(f32)]
    )
    kept = kept.reshape(4, 8, 4, 32).transpose(2, 0, 1, 3).reshape(4, 8, 128)
    kept = in_order(traded(kept, "y"), "y")
    kept = kept.reshape(4, 4, 8, 32).transpose(1, 0, 2, 3).reshape(2, LAYERS, 32, 32)
    window = jnp.concatenate([history[:, :, 1:], kept[1].astype(bf16)[:, :, None]], axis=2)
    return second.T, kept[0], window


def solution(mesh):
    torus = Mesh(mesh.devices.reshape(8, 2, 2, 4, 4, 2), AXES)
    in_specs = (
        P(None, DP + TP),
        P(DP),
        P(None, DP, TP),
        P(None, DP, None, TP),
        P(None, DP),
        P(None, DP, TP),
        P(None, DP, TP),
        P(None, None, TP),
        P(None, None, TP),
        P(None, None, TP),
        P(None, TP),
        P(None, TP, DP),
    )
    out_specs = (P(None, DP + TP), P(None, DP, TP), P(None, DP, None, TP))
    return jax.shard_map(
        both_blocks, mesh=torus, in_specs=in_specs, out_specs=out_specs, check_vma=False
    )
```

```python
import jax
import jax.numpy as jnp
from jax import lax
from jax.sharding import Mesh
from jax.sharding import PartitionSpec as P


D = 4096
BLOCK = 256
LAYERS = 2
TAPS = 4
AXES = ("zh", "zm", "zl", "y", "x", "core")
Z = ("zh", "zm", "zl")
ZQ = ("zm", "zl")
TP = ("zh", "zm", "zl", "y")
DP = ("x", "core")
PLANE = ("x", "core", "y")
PAIRED_PLANE = ("zl", "y", "x", "core")
bf16 = jnp.bfloat16
f32 = jnp.float32


epsilon = 1e-06


def exchange(tiles, axes):
    return lax.all_to_all(tiles, axes, 0, 0, tiled=True)


def everywhere(array, axes):
    count = lax.axis_size(axes)
    return exchange(jnp.broadcast_to(array[None], (count, *array.shape)), axes)


def passed(piece, axis, step):
    count = lax.axis_size(axis)
    return lax.ppermute(piece, axis, [(at, (at + step) % count) for at in range(count)])


def traded(tiles, axis):
    count = lax.axis_size(axis)
    here = lax.axis_index(axis)
    pieces = []
    for step in range(count):
        piece = lax.dynamic_slice_in_dim(tiles, (here + step) & 3, 1)[0]
        pieces.append(passed(piece, axis, step) if step else piece)
    return pieces


def counted_back(pieces, axis):
    here = lax.axis_index(axis)
    pieces = [pieces[-k % 4] for k in range(4)]
    pieces = [jnp.where((here & 1) == 1, pieces[k - 1], pieces[k]) for k in range(4)]
    return [jnp.where(here > 1, pieces[k - 2], pieces[k]) for k in range(4)]


def parts_of(value):
    coarse = lax.reduce_precision(value, 8, 7)
    rest = value - coarse
    middle = lax.reduce_precision(rest, 8, 7)
    return [coarse.astype(bf16), middle.astype(bf16), (rest - middle).astype(bf16)]


def whole_of(coarse, middle, fine):
    return coarse.astype(f32) + (middle.astype(f32) + fine.astype(f32))


def contract(a, a_dim, b, b_dim):
    return lax.dot_general(a, b, (((a_dim,), (b_dim,)), ((), ())), preferred_element_type=f32)


def grouped_features(rows_by_feature):
    width = rows_by_feature.shape[1]
    to = jnp.arange(width, dtype=jnp.int32)
    source = (to % 128) // 4 * 16 + to // 128 * 4 + to % 4
    chosen = (jnp.arange(width, dtype=jnp.int32)[:, None] == source[None, :]).astype(bf16)
    return contract(rows_by_feature, 1, chosen, 0).astype(bf16)


def gated_step(branch, gate_in, upper, history, taps, gates, decay, earlier):
    convolved = (
        jnp.sum(history * taps[:3, None], axis=0) + branch.astype(f32) * taps[3]
    ).astype(bf16)
    half = BLOCK // 2
    mapped = [
        contract(convolved[:, :half], 1, gates[kind, 0], 1)
        + contract(convolved[:, half:], 1, gates[kind, 1], 1)
        for kind in range(2)
    ]
    own = jnp.where(upper, convolved[:, half:], convolved[:, :half])
    input_gate = jax.nn.sigmoid(mapped[0])
    recur_gate = jax.nn.sigmoid(mapped[1])
    log_keep = 8.0 * recur_gate * decay
    keeping = jnp.exp(log_keep)
    feeding = jnp.sqrt(-jnp.expm1(2.0 * log_keep))
    state = keeping * earlier + feeding * input_gate * own.astype(f32)
    readout = (state * jax.nn.gelu(gate_in.astype(f32))).astype(bf16)
    own_branch = jnp.where(upper, branch[:, half:], branch[:, :half])
    return state, own_branch, readout


def both_blocks(
    stream,
    lengths,
    prior_state,
    prior_window,
    norm_gain,
    w_branch,
    w_gate_branch,
    conv_taps,
    w_in_gate,
    w_rec_gate,
    decay_param,
    w_out,
):
    zl = lax.axis_index("zl")
    upper = zl == 1

    stream_t = everywhere(stream.T, Z).reshape(128, 2, 128).transpose(1, 0, 2)

    def scaled(weight):
        return (weight.transpose(0, 2, 1).astype(f32) * norm_gain[:, None]).astype(bf16)

    by_feature = [
        grouped_features(weight.reshape(64, 512)).reshape(2, 32, 4, 128)
        for weight in (scaled(w_branch), scaled(w_gate_branch), w_out)
    ]
    w_first = jnp.concatenate([by_feature[0][0], by_feature[1][0]]).reshape(64, 512)
    place = lax.axis_index("y") * 128 + zl * 64 + lax.broadcasted_iota(jnp.int32, (64, 512), 0)
    kept_rows = (place == lax.broadcasted_iota(jnp.int32, (64, 512), 1)).astype(bf16)
    w_first = jnp.concatenate([w_first, kept_rows])
    second_weights = jnp.stack([by_feature[0][1], by_feature[1][1]])
    gate_rows = (
        jnp.stack([w_in_gate, w_rec_gate], axis=1)
        .reshape(LAYERS, 2, 2, 128, 32)
        .transpose(0, 1, 2, 4, 3)
        .reshape(256, 128)
    )
    depth = TAPS - 1
    needed = depth + 1 - jnp.arange(depth, dtype=jnp.int32)
    living = lengths[None, :, None, None] >= needed[None, None, :, None]
    history = jnp.where(living, prior_window, jnp.zeros_like(prior_window))
    earlier = jnp.where(
        lengths[None, :, None] >= 2, prior_state, jnp.zeros_like(prior_state)
    )
    earlier = earlier.reshape(LAYERS, 4, 8, 32).transpose(1, 0, 2, 3).reshape(4, -1)
    decay = jnp.broadcast_to(jax.nn.log_sigmoid(decay_param).reshape(1, -1), (4, 64))
    small = jnp.concatenate(
        parts_of(earlier) + parts_of(decay) + [jnp.zeros((4, 64), bf16)], axis=1
    ).reshape(4, 14, 128)
    windows = jnp.concatenate(
        [
            history.reshape(LAYERS, 4, 8, depth, 32).transpose(1, 0, 3, 2, 4).reshape(4, -1),
            jnp.broadcast_to(conv_taps.reshape(1, -1), (4, 256)),
        ],
        axis=1,
    ).reshape(4, 14, 128)

    def for_each(rows):
        return jnp.broadcast_to(rows.reshape(1, -1, 128), (4, rows.size // 128, 128))

    shared = jnp.concatenate(
        [
            by_feature[2][0].transpose(1, 0, 2),
            second_weights.transpose(2, 0, 1, 3).reshape(4, 64, 128),
            for_each(windows),
        ],
        axis=1,
    )
    shared = traded(shared, ZQ)
    partner = jnp.where(upper, shared[1][96:], shared[3][96:]).reshape(4, 14, 128)
    shared = counted_back([piece[:96] for piece in shared], ZQ)
    near = jnp.concatenate(
        [
            for_each(gate_rows[:128]),
            for_each(jnp.concatenate([piece[:32] for piece in shared])),
            small,
            jnp.where(upper, partner, windows),
            jnp.where(upper, windows, partner),
        ],
        axis=1,
    )
    near, w_first = lax.optimization_barrier((near, w_first))
    near = jnp.concatenate([for_each(stream_t), near], axis=1)
    near = exchange(near, "y")
    stream_t = near[:, :256].reshape(4, 2, 128, 128).transpose(1, 0, 2, 3).reshape(2, 512, 128)

    def gates_of(rows):
        return (
            rows.reshape(4, 2, 2, 32, 128).transpose(1, 2, 0, 3, 4).reshape(2, 2, 128, 128)
        )

    gates = gates_of(near[:, 256:384])
    w_mid = (
        near[:, 384:512].reshape(4, 4, 32, 128).transpose(1, 0, 2, 3).reshape(512, 128)
    )
    small = near[:, 512:526].reshape(4, 1792)
    windows = near[:, 526:].reshape(4, 2, 1792)
    later_rows = jnp.concatenate(
        [
            for_each(gate_rows[128:]),
            for_each(jnp.concatenate([piece[32:] for piece in shared])),
            by_feature[2][1].transpose(1, 0, 2),
        ],
        axis=1,
    )
    later_rows = jnp.stack(counted_back(traded(later_rows, "y"), "y"))
    gates_second = gates_of(later_rows[:, :128])
    w_second = (
        later_rows[:, 128:384]
        .reshape(4, 4, 2, 32, 128)
        .transpose(1, 2, 0, 3, 4)
        .reshape(1024, 128)
    )
    w_last = later_rows[:, 384:].reshape(128, 128)

    earlier_rows = (
        whole_of(small[:, :512], small[:, 512:1024], small[:, 1024:1536])
        .reshape(4, LAYERS, 8, 32)
        .transpose(1, 2, 0, 3)
        .reshape(LAYERS, 8, 128)
    )
    decay = (
        whole_of(small[:, 1536:1600], small[:, 1600:1664], small[:, 1664:1728])
        .reshape(4, LAYERS, 32)
        .transpose(1, 0, 2)
        .reshape(LAYERS, 1, 128)
    )
    history_rows = (
        windows[:, :, :1536]
        .reshape(4, 2, LAYERS * depth * 8, 32)
        .transpose(2, 1, 0, 3)
        .reshape(LAYERS, depth, 8, 256)
        .astype(f32)
    )
    taps = (
        windows[:, :, 1536:]
        .reshape(4, 2, LAYERS * TAPS, 32)
        .transpose(2, 1, 0, 3)
        .reshape(LAYERS, TAPS, 256)
        .astype(f32)
    )

    products = jnp.concatenate(
        [contract(stream_t[half], 0, w_first, 1).astype(bf16) for half in range(2)]
    )
    products = products.reshape(8, 4, 8, 128).transpose(1, 0, 2, 3).reshape(1, 32, 8, 128)
    sent = jnp.broadcast_to(products, (2, 32, 8, 128)).reshape(64, 8, 128)
    came = exchange(sent, PAIRED_PLANE).reshape(2, 4, 8, 8, 128)
    later = (history_rows[1], taps[1], decay[1], earlier_rows[1], history)
    came, w_mid, later = lax.optimization_barrier((came, w_mid, later))
    summed = came.astype(f32).sum(axis=2)
    branch = summed[:, :, :, :32].transpose(2, 0, 1, 3).reshape(8, 256)
    gate_in = jnp.where(upper, summed[1], summed[0])[:, :, 32:64].transpose(1, 0, 2).reshape(8, 128)
    rows = came[:, :, :, :, 64:]
    widened = rows.astype(f32)
    squares = jnp.sum(widened * widened, axis=(0, 1, 2, 4))[:, None]
    rows = jnp.concatenate([rows[0], rows[1]], axis=3).reshape(32, 8, 128)
    scaling = lax.rsqrt(squares / D + epsilon)
    state_first, branch_first, readout = gated_step(
        (branch * scaling).astype(bf16),
        (gate_in * scaling).astype(bf16),
        upper,
        history_rows[0],
        taps[0],
        gates,
        decay[0],
        earlier_rows[0],
    )
    sent = jnp.stack([jnp.broadcast_to(readout[None], (32, 8, 128)), rows], axis=1)
    came = exchange(sent.reshape(32, 16, 128), ZQ + DP).reshape(4, 8, 2, 8, 128)
    residual = came[0, :, 1].reshape(64, 128).astype(f32)
    came = came[:, :, 0].reshape(4, 64, 128)
    came = jnp.concatenate([came[at] for at in range(4)], axis=1)
    mixed = contract(came, 1, w_mid, 0).astype(bf16)
    mixed = everywhere(mixed, "zh")
    mixed, w_second, gates_second, w_last = lax.optimization_barrier(
        (mixed, w_second, gates_second, w_last)
    )
    mixed = mixed.astype(f32).sum(axis=0)
    first = (mixed + residual).astype(bf16)

    products = contract(first, 1, w_second, 1).astype(bf16)
    products = [products[:, 128 * at : 128 * (at + 1)].reshape(8, 8, 128) for at in range(8)]
    own_rows = first.reshape(8, 8, 128)
    sent = jnp.stack(
        [
            jnp.stack(
                [
                    products[4 * zm],
                    products[4 * zm + 2],
                    products[4 * zm + 2 * low + 1],
                    own_rows,
                ],
                axis=1,
            )
            for zm in range(2)
            for low in range(2)
        ]
    )
    came = exchange(sent.reshape(32, 32, 128), ZQ + DP).reshape(32, 4, 8, 128)
    rows = came[:, 3]
    came = came[:, :3].astype(f32).sum(axis=0)
    widened = rows.astype(f32)
    squares = jnp.sum(jnp.sum(widened * widened, axis=0), axis=1, keepdims=True)
    branch = jnp.concatenate([came[0], came[1]], axis=1)
    scaling = lax.rsqrt(squares / D + epsilon)
    state_second, branch_second, readout = gated_step(
        (branch * scaling).astype(bf16),
        (came[2] * scaling).astype(bf16),
        upper,
        later[0],
        later[1],
        gates_second,
        later[2],
        later[3],
    )
    sent = jnp.stack(
        [
            jnp.broadcast_to(readout[None], (32, 8, 128)),
            rows.reshape(4, 8, 8, 128).transpose(1, 0, 2, 3).reshape(32, 8, 128),
        ],
        axis=1,
    )
    came = exchange(sent.reshape(32, 16, 128), PLANE).reshape(32, 2, 8, 128)
    mixed = contract(w_last, 0, came[:, 0].reshape(256, 128), 1).astype(bf16)
    mixed = mixed.reshape(32, 4, 256)
    own = lax.broadcasted_iota(jnp.int32, (4, 128), 0) + 4 * lax.axis_index(Z)
    own = (own == lax.broadcasted_iota(jnp.int32, (4, 128), 1)).astype(bf16)
    residual = contract(own, 1, came[:, 1].reshape(256, 128), 1)
    second = exchange(mixed, Z).astype(f32).sum(axis=0)
    second = (second + residual).astype(bf16)

    kept = jnp.stack(
        [state_first, state_second, branch_first.astype(f32), branch_second.astype(f32)]
    )
    kept = kept.reshape(4, 8, 4, 32).transpose(2, 0, 1, 3).reshape(4, 8, 128)
    kept = jnp.stack(counted_back(traded(kept, "y"), "y"))
    kept = kept.reshape(4, 4, 8, 32).transpose(1, 0, 2, 3).reshape(2, LAYERS, 32, 32)
    window = jnp.concatenate([later[4][:, :, 1:], kept[1].astype(bf16)[:, :, None]], axis=2)
    return second.T, kept[0], window


def solution(mesh):
    torus = Mesh(mesh.devices.reshape(8, 2, 2, 4, 4, 2), AXES)
    in_specs = (
        P(None, DP + TP),
        P(DP),
        P(None, DP, TP),
        P(None, DP, None, TP),
        P(None, DP),
        P(None, DP, TP),
        P(None, DP, TP),
        P(None, None, TP),
        P(None, None, TP),
        P(None, None, TP),
        P(None, TP),
        P(None, TP, DP),
    )
    out_specs = (P(None, DP + TP), P(None, DP, TP), P(None, DP, None, TP))
    return jax.shard_map(
        both_blocks, mesh=torus, in_specs=in_specs, out_specs=out_specs, check_vma=False
    )
```

```python
import jax
import jax.numpy as jnp
from jax import lax
from jax.sharding import Mesh
from jax.sharding import PartitionSpec as P


D = 4096
BLOCK = 256
LAYERS = 2
TAPS = 4
AXES = ("zh", "zm", "zl", "y", "x", "core")
Z = ("zh", "zm", "zl")
ZQ = ("zm", "zl")
TP = ("zh", "zm", "zl", "y")
DP = ("x", "core")
PLANE = ("x", "core", "y")
PAIRED_PLANE = ("zl", "y", "x", "core")
bf16 = jnp.bfloat16
f32 = jnp.float32


epsilon = 1e-06


def exchange(tiles, axes):
    return lax.all_to_all(tiles, axes, 0, 0, tiled=True)


def exchange_far(tiles, axes):
    count = lax.axis_size(axes)
    first = count * 3 // 4
    order = [(first + at) % count for at in range(count)]
    tiles = lax.all_to_all(
        jnp.roll(tiles, -first, axis=0), axes, 0, 0, axis_index_groups=[order], tiled=True
    )
    return jnp.roll(tiles, first, axis=0)


def everywhere(array, axes):
    count = lax.axis_size(axes)
    tiles = jnp.broadcast_to(array[None], (count, *array.shape))
    return exchange_far(tiles, axes)


def passed(piece, axis, step):
    count = lax.axis_size(axis)
    return lax.ppermute(piece, axis, [(at, (at + step) % count) for at in range(count)])


def traded(tiles, axis):
    count = lax.axis_size(axis)
    here = lax.axis_index(axis)
    pieces = []
    for step in range(count):
        piece = lax.dynamic_slice_in_dim(tiles, (here + step) & 3, 1)[0]
        pieces.append(passed(piece, axis, step) if step else piece)
    return pieces


def counted_back(pieces, axis):
    here = lax.axis_index(axis)
    pieces = [pieces[-k % 4] for k in range(4)]
    pieces = [jnp.where((here & 1) == 1, pieces[k - 1], pieces[k]) for k in range(4)]
    return [jnp.where(here > 1, pieces[k - 2], pieces[k]) for k in range(4)]


def parts_of(value):
    coarse = lax.reduce_precision(value, 8, 7)
    rest = value - coarse
    middle = lax.reduce_precision(rest, 8, 7)
    return [coarse.astype(bf16), middle.astype(bf16), (rest - middle).astype(bf16)]


def whole_of(coarse, middle, fine):
    return coarse.astype(f32) + (middle.astype(f32) + fine.astype(f32))


def contract(a, a_dim, b, b_dim):
    return lax.dot_general(a, b, (((a_dim,), (b_dim,)), ((), ())), preferred_element_type=f32)


def grouped_features(rows_by_feature):
    width = rows_by_feature.shape[1]
    to = jnp.arange(width, dtype=jnp.int32)
    source = (to % 128) // 4 * 16 + to // 128 * 4 + to % 4
    chosen = (jnp.arange(width, dtype=jnp.int32)[:, None] == source[None, :]).astype(bf16)
    return contract(rows_by_feature, 1, chosen, 0).astype(bf16)


def gated_step(branch, gate_in, upper, history, taps, gates, decay, earlier):
    convolved = (
        jnp.sum(history * taps[:3, None], axis=0) + branch.astype(f32) * taps[3]
    ).astype(bf16)
    half = BLOCK // 2
    mapped = [
        contract(convolved[:, :half], 1, gates[kind, 0], 1)
        + contract(convolved[:, half:], 1, gates[kind, 1], 1)
        for kind in range(2)
    ]
    own = jnp.where(upper, convolved[:, half:], convolved[:, :half])
    input_gate = jax.nn.sigmoid(mapped[0])
    recur_gate = jax.nn.sigmoid(mapped[1])
    log_keep = 8.0 * recur_gate * decay
    keeping = jnp.exp(log_keep)
    feeding = jnp.sqrt(-jnp.expm1(2.0 * log_keep))
    state = keeping * earlier + feeding * input_gate * own.astype(f32)
    readout = (state * jax.nn.gelu(gate_in.astype(f32))).astype(bf16)
    own_branch = jnp.where(upper, branch[:, half:], branch[:, :half])
    return state, own_branch, readout


def both_blocks(
    stream,
    lengths,
    prior_state,
    prior_window,
    norm_gain,
    w_branch,
    w_gate_branch,
    conv_taps,
    w_in_gate,
    w_rec_gate,
    decay_param,
    w_out,
):
    zl = lax.axis_index("zl")
    upper = zl == 1

    stream_t = everywhere(stream.T, Z).reshape(128, 2, 128).transpose(1, 0, 2)

    def scaled(weight):
        return (weight.transpose(0, 2, 1).astype(f32) * norm_gain[:, None]).astype(bf16)

    by_feature = [
        grouped_features(weight.reshape(64, 512)).reshape(2, 32, 4, 128)
        for weight in (scaled(w_branch), scaled(w_gate_branch), w_out)
    ]
    w_first = jnp.concatenate([by_feature[0][0], by_feature[1][0]]).reshape(64, 512)
    place = lax.axis_index("y") * 128 + zl * 64 + lax.broadcasted_iota(jnp.int32, (64, 512), 0)
    kept_rows = (place == lax.broadcasted_iota(jnp.int32, (64, 512), 1)).astype(bf16)
    w_first = jnp.concatenate([w_first, kept_rows])
    second_weights = jnp.stack([by_feature[0][1], by_feature[1][1]])
    gate_rows = (
        jnp.stack([w_in_gate, w_rec_gate], axis=1)
        .reshape(LAYERS, 2, 2, 128, 32)
        .transpose(0, 1, 2, 4, 3)
        .reshape(256, 128)
    )
    depth = TAPS - 1
    needed = depth + 1 - jnp.arange(depth, dtype=jnp.int32)
    living = lengths[None, :, None, None] >= needed[None, None, :, None]
    history = jnp.where(living, prior_window, jnp.zeros_like(prior_window))
    earlier = jnp.where(
        lengths[None, :, None] >= 2, prior_state, jnp.zeros_like(prior_state)
    )
    earlier = earlier.reshape(LAYERS, 4, 8, 32).transpose(1, 0, 2, 3).reshape(4, -1)
    decay = jnp.broadcast_to(jax.nn.log_sigmoid(decay_param).reshape(1, -1), (4, 64))
    small = jnp.concatenate(
        parts_of(earlier) + parts_of(decay) + [jnp.zeros((4, 64), bf16)], axis=1
    ).reshape(4, 14, 128)
    windows = jnp.concatenate(
        [
            history.reshape(LAYERS, 4, 8, depth, 32).transpose(1, 0, 3, 2, 4).reshape(4, -1),
            jnp.broadcast_to(conv_taps.reshape(1, -1), (4, 256)),
        ],
        axis=1,
    ).reshape(4, 14, 128)

    def for_each(rows):
        return jnp.broadcast_to(rows.reshape(1, -1, 128), (4, rows.size // 128, 128))

    shared = jnp.concatenate(
        [
            by_feature[2][0].transpose(1, 0, 2),
            second_weights.transpose(2, 0, 1, 3).reshape(4, 64, 128),
            for_each(windows),
        ],
        axis=1,
    )
    shared = traded(shared, ZQ)
    partner = jnp.where(upper, shared[1][96:], shared[3][96:]).reshape(4, 14, 128)
    shared = counted_back([piece[:96] for piece in shared], ZQ)
    near = jnp.concatenate(
        [
            for_each(gate_rows[:128]),
            for_each(jnp.concatenate([piece[:32] for piece in shared])),
            small,
            jnp.where(upper, partner, windows),
            jnp.where(upper, windows, partner),
        ],
        axis=1,
    )
    near, w_first = lax.optimization_barrier((near, w_first))
    near = jnp.concatenate([for_each(stream_t), near], axis=1)
    near = exchange(near, "y")
    stream_t = near[:, :256].reshape(4, 2, 128, 128).transpose(1, 0, 2, 3).reshape(2, 512, 128)

    def gates_of(rows):
        return (
            rows.reshape(4, 2, 2, 32, 128).transpose(1, 2, 0, 3, 4).reshape(2, 2, 128, 128)
        )

    gates = gates_of(near[:, 256:384])
    w_mid = (
        near[:, 384:512].reshape(4, 4, 32, 128).transpose(1, 0, 2, 3).reshape(512, 128)
    )
    small = near[:, 512:526].reshape(4, 1792)
    windows = near[:, 526:].reshape(4, 2, 1792)
    later_rows = jnp.concatenate(
        [
            for_each(gate_rows[128:]),
            for_each(jnp.concatenate([piece[32:] for piece in shared])),
            by_feature[2][1].transpose(1, 0, 2),
        ],
        axis=1,
    )
    later_rows = jnp.stack(counted_back(traded(later_rows, "y"), "y"))
    gates_second = gates_of(later_rows[:, :128])
    w_second = (
        later_rows[:, 128:384]
        .reshape(4, 4, 2, 32, 128)
        .transpose(1, 2, 0, 3, 4)
        .reshape(1024, 128)
    )
    w_last = later_rows[:, 384:].reshape(128, 128)

    earlier_rows = (
        whole_of(small[:, :512], small[:, 512:1024], small[:, 1024:1536])
        .reshape(4, LAYERS, 8, 32)
        .transpose(1, 2, 0, 3)
        .reshape(LAYERS, 8, 128)
    )
    decay = (
        whole_of(small[:, 1536:1600], small[:, 1600:1664], small[:, 1664:1728])
        .reshape(4, LAYERS, 32)
        .transpose(1, 0, 2)
        .reshape(LAYERS, 1, 128)
    )
    history_rows = (
        windows[:, :, :1536]
        .reshape(4, 2, LAYERS * depth * 8, 32)
        .transpose(2, 1, 0, 3)
        .reshape(LAYERS, depth, 8, 256)
        .astype(f32)
    )
    taps = (
        windows[:, :, 1536:]
        .reshape(4, 2, LAYERS * TAPS, 32)
        .transpose(2, 1, 0, 3)
        .reshape(LAYERS, TAPS, 256)
        .astype(f32)
    )

    products = jnp.concatenate(
        [contract(stream_t[half], 0, w_first, 1).astype(bf16) for half in range(2)]
    )
    products = products.reshape(8, 4, 8, 128).transpose(1, 0, 2, 3).reshape(1, 32, 8, 128)
    sent = jnp.broadcast_to(products, (2, 32, 8, 128)).reshape(64, 8, 128)
    came = exchange(sent, PAIRED_PLANE).reshape(2, 4, 8, 8, 128)
    later = (history_rows[1], taps[1], decay[1], earlier_rows[1], history)
    came, w_mid, later = lax.optimization_barrier((came, w_mid, later))
    summed = came.astype(f32).sum(axis=2)
    branch = summed[:, :, :, :32].transpose(2, 0, 1, 3).reshape(8, 256)
    gate_in = jnp.where(upper, summed[1], summed[0])[:, :, 32:64].transpose(1, 0, 2).reshape(8, 128)
    rows = came[:, :, :, :, 64:]
    widened = rows.astype(f32)
    squares = jnp.sum(widened * widened, axis=(0, 1, 2, 4))[:, None]
    rows = jnp.concatenate([rows[0], rows[1]], axis=3).reshape(32, 8, 128)
    scaling = lax.rsqrt(squares / D + epsilon)
    state_first, branch_first, readout = gated_step(
        (branch * scaling).astype(bf16),
        (gate_in * scaling).astype(bf16),
        upper,
        history_rows[0],
        taps[0],
        gates,
        decay[0],
        earlier_rows[0],
    )
    sent = jnp.stack([jnp.broadcast_to(readout[None], (32, 8, 128)), rows], axis=1)
    came = exchange(sent.reshape(32, 16, 128), ZQ + DP).reshape(4, 8, 2, 8, 128)
    residual = came[0, :, 1].reshape(64, 128).astype(f32)
    came = came[:, :, 0].reshape(4, 64, 128)
    came = jnp.concatenate([came[at] for at in range(4)], axis=1)
    mixed = contract(came, 1, w_mid, 0).astype(bf16)
    mixed = everywhere(mixed, "zh")
    mixed, w_second, gates_second, w_last = lax.optimization_barrier(
        (mixed, w_second, gates_second, w_last)
    )
    mixed = mixed.astype(f32).sum(axis=0)
    first = (mixed + residual).astype(bf16)

    products = contract(first, 1, w_second, 1).astype(bf16)
    products = [products[:, 128 * at : 128 * (at + 1)].reshape(8, 8, 128) for at in range(8)]
    own_rows = first.reshape(8, 8, 128)
    sent = jnp.stack(
        [
            jnp.stack(
                [
                    products[4 * zm],
                    products[4 * zm + 2],
                    products[4 * zm + 2 * low + 1],
                    own_rows,
                ],
                axis=1,
            )
            for zm in range(2)
            for low in range(2)
        ]
    )
    came = exchange(sent.reshape(32, 32, 128), ZQ + DP).reshape(32, 4, 8, 128)
    rows = came[:, 3]
    came = came[:, :3].astype(f32).sum(axis=0)
    widened = rows.astype(f32)
    squares = jnp.sum(jnp.sum(widened * widened, axis=0), axis=1, keepdims=True)
    branch = jnp.concatenate([came[0], came[1]], axis=1)
    scaling = lax.rsqrt(squares / D + epsilon)
    state_second, branch_second, readout = gated_step(
        (branch * scaling).astype(bf16),
        (came[2] * scaling).astype(bf16),
        upper,
        later[0],
        later[1],
        gates_second,
        later[2],
        later[3],
    )
    sent = jnp.stack(
        [
            jnp.broadcast_to(readout[None], (32, 8, 128)),
            rows.reshape(4, 8, 8, 128).transpose(1, 0, 2, 3).reshape(32, 8, 128),
        ],
        axis=1,
    )
    came = exchange(sent.reshape(32, 16, 128), PLANE).reshape(32, 2, 8, 128)
    mixed = contract(w_last, 0, came[:, 0].reshape(256, 128), 1).astype(bf16)
    mixed = mixed.reshape(32, 4, 256)
    own = lax.broadcasted_iota(jnp.int32, (4, 128), 0) + 4 * lax.axis_index(Z)
    own = (own == lax.broadcasted_iota(jnp.int32, (4, 128), 1)).astype(bf16)
    residual = contract(own, 1, came[:, 1].reshape(256, 128), 1)
    second = exchange_far(mixed, Z).astype(f32).sum(axis=0)
    second = (second + residual).astype(bf16)

    kept = jnp.stack(
        [state_first, state_second, branch_first.astype(f32), branch_second.astype(f32)]
    )
    kept = kept.reshape(4, 8, 4, 32).transpose(2, 0, 1, 3).reshape(4, 8, 128)
    kept = jnp.stack(counted_back(traded(kept, "y"), "y"))
    kept = kept.reshape(4, 4, 8, 32).transpose(1, 0, 2, 3).reshape(2, LAYERS, 32, 32)
    window = jnp.concatenate([later[4][:, :, 1:], kept[1].astype(bf16)[:, :, None]], axis=2)
    return second.T, kept[0], window


def solution(mesh):
    torus = Mesh(mesh.devices.reshape(8, 2, 2, 4, 4, 2), AXES)
    in_specs = (
        P(None, DP + TP),
        P(DP),
        P(None, DP, TP),
        P(None, DP, None, TP),
        P(None, DP),
        P(None, DP, TP),
        P(None, DP, TP),
        P(None, None, TP),
        P(None, None, TP),
        P(None, None, TP),
        P(None, TP),
        P(None, TP, DP),
    )
    out_specs = (P(None, DP + TP), P(None, DP, TP), P(None, DP, None, TP))
    return jax.shard_map(
        both_blocks, mesh=torus, in_specs=in_specs, out_specs=out_specs, check_vma=False
    )
```

```python
import jax
import jax.numpy as jnp
from jax import lax
from jax.sharding import Mesh
from jax.sharding import PartitionSpec as P


D = 4096
BLOCK = 256
LAYERS = 2
TAPS = 4
AXES = ("zh", "zm", "zl", "y", "x", "core")
Z = ("zh", "zm", "zl")
ZQ = ("zm", "zl")
TP = ("zh", "zm", "zl", "y")
DP = ("x", "core")
PLANE = ("x", "core", "y")
PAIRED_PLANE = ("zl", "y", "x", "core")
FIRST_GATHER = 24
FIRST_REDUCE = 4
FIRST_LAST = 20
bf16 = jnp.bfloat16
f32 = jnp.float32


epsilon = 1e-06


def exchange(tiles, axes):
    return lax.all_to_all(tiles, axes, 0, 0, tiled=True)


def exchange_far(tiles, axes, first):
    count = lax.axis_size(axes)
    order = [(first + at) % count for at in range(count)]
    return lax.all_to_all(tiles, axes, 0, 0, axis_index_groups=[order], tiled=True)


def everywhere(array, axes, first):
    count = lax.axis_size(axes)
    tiles = jnp.broadcast_to(array[None], (count, *array.shape))
    return exchange_far(tiles, axes, first)


def passed(piece, axis, flip):
    return lax.ppermute(piece, axis, [(at, at ^ flip) for at in range(lax.axis_size(axis))])


def traded(tiles, axis):
    here = lax.axis_index(axis)
    pieces = [lax.dynamic_slice_in_dim(tiles, here ^ flip, 1)[0] for flip in range(4)]
    return pieces[:1] + [passed(pieces[flip], axis, flip) for flip in range(1, 4)]


def in_order(pieces, axis):
    here = lax.axis_index(axis)
    pieces = [jnp.where((here & 1) == 1, pieces[k ^ 1], pieces[k]) for k in range(4)]
    return [jnp.where(here > 1, pieces[k ^ 2], pieces[k]) for k in range(4)]


def parts_of(value):
    coarse = lax.reduce_precision(value, 8, 7)
    rest = value - coarse
    middle = lax.reduce_precision(rest, 8, 7)
    return [coarse.astype(bf16), middle.astype(bf16), (rest - middle).astype(bf16)]


def whole_of(coarse, middle, fine):
    return coarse.astype(f32) + (middle.astype(f32) + fine.astype(f32))


def contract(a, a_dim, b, b_dim):
    return lax.dot_general(a, b, (((a_dim,), (b_dim,)), ((), ())), preferred_element_type=f32)


def grouped_features(rows_by_feature, first):
    width = rows_by_feature.shape[1]
    to = jnp.arange(width, dtype=jnp.int32)
    source = ((to % 128) // 4 + first) % 32 * 16 + to // 128 * 4 + to % 4
    chosen = (jnp.arange(width, dtype=jnp.int32)[:, None] == source[None, :]).astype(bf16)
    return contract(rows_by_feature, 1, chosen, 0).astype(bf16)


def gated_step(branch, gate_in, upper, history, taps, gates, decay, earlier):
    convolved = (
        jnp.sum(history * taps[:3, None], axis=0) + branch.astype(f32) * taps[3]
    ).astype(bf16)
    half = BLOCK // 2
    mapped = [
        contract(convolved[:, :half], 1, gates[kind, 0], 1)
        + contract(convolved[:, half:], 1, gates[kind, 1], 1)
        for kind in range(2)
    ]
    own = jnp.where(upper, convolved[:, half:], convolved[:, :half])
    input_gate = jax.nn.sigmoid(mapped[0])
    recur_gate = jax.nn.sigmoid(mapped[1])
    log_keep = 8.0 * recur_gate * decay
    keeping = jnp.exp(log_keep)
    feeding = jnp.sqrt(-jnp.expm1(2.0 * log_keep))
    state = keeping * earlier + feeding * input_gate * own.astype(f32)
    readout = (state * jax.nn.gelu(gate_in.astype(f32))).astype(bf16)
    own_branch = jnp.where(upper, branch[:, half:], branch[:, :half])
    return state, own_branch, readout


def both_blocks(
    stream,
    lengths,
    prior_state,
    prior_window,
    norm_gain,
    w_branch,
    w_gate_branch,
    conv_taps,
    w_in_gate,
    w_rec_gate,
    decay_param,
    w_out,
):
    zl = lax.axis_index("zl")
    upper = zl == 1

    stream_t = everywhere(stream.T, Z, FIRST_GATHER).reshape(128, 2, 128).transpose(1, 0, 2)

    def by_quarter(weight):
        return weight.reshape(32, 4, 128).transpose(1, 0, 2)

    gate_rows = (
        jnp.stack([w_in_gate, w_rec_gate], axis=1)
        .reshape(LAYERS, 2, 2, 128, 32)
        .transpose(0, 1, 2, 4, 3)
        .reshape(256, 128)
    )
    depth = TAPS - 1
    needed = depth + 1 - jnp.arange(depth, dtype=jnp.int32)
    living = lengths[None, :, None, None] >= needed[None, None, :, None]
    history = jnp.where(living, prior_window, jnp.zeros_like(prior_window))
    earlier = jnp.where(
        lengths[None, :, None] >= 2, prior_state, jnp.zeros_like(prior_state)
    )

    def by_rows(groups):
        packed = jnp.concatenate(groups, axis=1).reshape(4, 8, -1, 128)
        return packed.transpose(0, 2, 1, 3).reshape(4, -1, 128)

    def for_all(rows):
        return jnp.broadcast_to(rows[None], (4, 8, 32)).reshape(32, 32)

    decay = jnp.concatenate(
        parts_of(jax.nn.log_sigmoid(decay_param)) + [jnp.zeros((2, 32), bf16)]
    )
    none = jnp.zeros((32, 32), bf16)
    small = by_rows(
        [part[layer] for layer in range(LAYERS) for part in parts_of(earlier)]
        + [for_all(decay), none]
    )
    windows = by_rows(
        [history[layer, :, tap] for layer in range(LAYERS) for tap in range(depth)]
        + [for_all(conv_taps.reshape(8, 32)), none]
    )

    def for_each(rows):
        return jnp.broadcast_to(rows.reshape(1, -1, 128), (4, rows.size // 128, 128))

    shared = jnp.concatenate(
        [
            by_quarter(w_out[0]),
            by_quarter(w_branch[1].T),
            by_quarter(w_gate_branch[1].T),
            for_each(windows),
        ],
        axis=1,
    )
    shared = traded(shared, ZQ)
    partner = shared[1][96:].reshape(4, 16, 128)
    shared = in_order([piece[:96] for piece in shared], ZQ)
    near = jnp.concatenate(
        [
            for_each(gate_rows[:128]),
            for_each(jnp.concatenate([piece[:32] for piece in shared])),
            small,
            jnp.where(upper, partner, windows),
            jnp.where(upper, windows, partner),
        ],
        axis=1,
    )
    stream_t, near, first_weights = lax.optimization_barrier(
        (stream_t, near, (w_branch[0], w_gate_branch[0], norm_gain[0]))
    )
    near = jnp.concatenate([for_each(stream_t), near], axis=1)
    near = exchange(near, "y")
    w_first = jnp.concatenate([first_weights[0].T, first_weights[1].T]).astype(f32)
    w_first = grouped_features((w_first * first_weights[2]).astype(bf16), FIRST_GATHER)
    place = (zl * 4 + lax.axis_index("y")) * 64 + lax.broadcasted_iota(jnp.int32, (64, 512), 0)
    place = (place % 16) // 4 * 128 + (place // 16 - FIRST_GATHER) % 32 * 4 + place % 4
    kept_rows = (place == lax.broadcasted_iota(jnp.int32, (64, 512), 1)).astype(bf16)
    w_first = jnp.concatenate([w_first, kept_rows])
    stream_t = near[:, :256].reshape(4, 2, 128, 128).transpose(1, 0, 2, 3).reshape(2, 512, 128)

    def gates_of(rows):
        return (
            rows.reshape(4, 2, 2, 32, 128).transpose(1, 2, 0, 3, 4).reshape(2, 2, 128, 128)
        )

    gates = gates_of(near[:, 256:384])
    w_mid = (
        near[:, 384:512].reshape(4, 4, 32, 128).transpose(1, 0, 2, 3).reshape(512, 128)
    )
    groups = near[:, 512:].reshape(4, 6, 8, 4, 32).transpose(1, 3, 2, 0, 4).reshape(24, 8, 128)
    windows = jnp.concatenate([groups[8:16], groups[16:]], axis=2).astype(f32)
    later_rows = jnp.concatenate(
        [
            for_each(gate_rows[128:]),
            for_each(jnp.concatenate([piece[32:] for piece in shared])),
            by_quarter(grouped_features(w_out[1], FIRST_LAST)),
        ],
        axis=1,
    )
    later_rows = jnp.stack(in_order(traded(later_rows, "y"), "y"))
    gates_second = gates_of(later_rows[:, :128])
    w_second = (
        later_rows[:, 128:384]
        .reshape(4, 4, 2, 32, 128)
        .transpose(1, 2, 0, 3, 4)
        .reshape(1024, 128)
    )
    w_last = later_rows[:, 384:].reshape(128, 128)

    earlier_rows = [whole_of(*groups[3 * layer : 3 * layer + 3]) for layer in range(LAYERS)]
    decay = whole_of(groups[6][:2], groups[6][2:4], groups[6][4:6])[:, None]
    history_rows = windows[:6].reshape(LAYERS, depth, 8, 256)
    taps = windows[6].reshape(LAYERS, TAPS, 256)

    products = jnp.concatenate(
        [contract(stream_t[half], 0, w_first, 1).astype(bf16) for half in range(2)]
    )
    products = products.reshape(8, 4, 8, 128).transpose(1, 0, 2, 3).reshape(1, 32, 8, 128)
    sent = jnp.broadcast_to(products, (2, 32, 8, 128)).reshape(64, 8, 128)
    came = exchange(sent, PAIRED_PLANE).reshape(2, 4, 8, 8, 128)
    later = (history_rows[1], taps[1], decay[1], earlier_rows[1], history)
    came, w_mid, later = lax.optimization_barrier((came, w_mid, later))
    summed = came.astype(f32).sum(axis=2)
    branch = summed[:, :, :, :32].transpose(2, 0, 1, 3).reshape(8, 256)
    gate_in = jnp.where(upper, summed[1], summed[0])[:, :, 32:64].transpose(1, 0, 2).reshape(8, 128)
    rows = came[:, :, :, :, 64:]
    widened = rows.astype(f32)
    squares = jnp.sum(widened * widened, axis=(0, 1, 2, 4))[:, None]
    rows = rows.reshape(4, 2, 8, 8, 64)
    rows = jnp.concatenate([rows[:, 0], rows[:, 1]], axis=3).reshape(32, 8, 128)
    scaling = lax.rsqrt(squares / D + epsilon)
    state_first, branch_first, readout = gated_step(
        (branch * scaling).astype(bf16),
        (gate_in * scaling).astype(bf16),
        upper,
        history_rows[0],
        taps[0],
        gates,
        decay[0],
        earlier_rows[0],
    )
    sent = jnp.stack([jnp.broadcast_to(readout[None], (32, 8, 128)), rows], axis=1)
    came = exchange(sent.reshape(32, 16, 128), ZQ + DP).reshape(4, 8, 2, 8, 128)
    residual = came[0, :, 1].reshape(64, 128).astype(f32)
    came = came[:, :, 0].reshape(4, 64, 128)
    came = jnp.concatenate([came[at] for at in range(4)], axis=1)
    mixed = contract(came, 1, w_mid, 0).astype(bf16)
    mixed = everywhere(mixed, "zh", FIRST_REDUCE)
    mixed, w_second, gates_second, w_last = lax.optimization_barrier(
        (mixed, w_second, gates_second, w_last)
    )
    mixed = mixed.astype(f32).sum(axis=0)
    first = (mixed + residual).astype(bf16)

    gain = lax.dynamic_slice_in_dim(norm_gain[1], lax.axis_index(ZQ) * 128, 128)
    scaled = (first.astype(f32) * gain).astype(bf16)
    products = contract(scaled, 1, w_second, 1).astype(bf16)
    products = [products[:, 128 * at : 128 * (at + 1)].reshape(8, 8, 128) for at in range(8)]
    own_rows = first.reshape(8, 8, 128)
    sent = jnp.stack(
        [
            jnp.stack(
                [
                    products[4 * zm],
                    products[4 * zm + 2],
                    products[4 * zm + 2 * low + 1],
                    own_rows,
                ],
                axis=1,
            )
            for zm in range(2)
            for low in range(2)
        ]
    )
    came = exchange(sent.reshape(32, 32, 128), ZQ + DP).reshape(32, 4, 8, 128)
    rows = came[:, 3]
    came = came[:, :3].astype(f32).sum(axis=0)
    widened = rows.astype(f32)
    squares = jnp.sum(jnp.sum(widened * widened, axis=0), axis=1, keepdims=True)
    branch = jnp.concatenate([came[0], came[1]], axis=1)
    scaling = lax.rsqrt(squares / D + epsilon)
    state_second, branch_second, readout = gated_step(
        (branch * scaling).astype(bf16),
        (came[2] * scaling).astype(bf16),
        upper,
        later[0],
        later[1],
        gates_second,
        later[2],
        later[3],
    )
    rows = lax.dynamic_slice_in_dim(rows.reshape(4, 8, 1, 8, 128), lax.axis_index("zh") // 2, 1)
    sent = jnp.stack(
        [
            jnp.broadcast_to(readout[None], (32, 8, 128)),
            jnp.broadcast_to(rows[0], (8, 4, 8, 128)).reshape(32, 8, 128),
        ],
        axis=1,
    )
    came = exchange(sent.reshape(32, 16, 128), PLANE).reshape(32, 2, 8, 128)
    mixed = contract(w_last, 0, came[:, 0].reshape(256, 128), 1).astype(bf16)
    mixed = mixed.reshape(32, 4, 256)
    own = (lax.axis_index(Z) & 7) * 16 + lax.axis_index("y") * 4
    own = lax.broadcasted_iota(jnp.int32, (4, 128), 0) + own
    own = (own == lax.broadcasted_iota(jnp.int32, (4, 128), 1)).astype(bf16)
    residual = contract(own, 1, came[:, 1].reshape(256, 128), 1)
    second = exchange_far(mixed, Z, FIRST_LAST).astype(f32).sum(axis=0)
    second = (second + residual).astype(bf16)

    kept = jnp.stack(
        [state_first, state_second, branch_first.astype(f32), branch_second.astype(f32)]
    )
    kept = kept.reshape(4, 8, 4, 32).transpose(2, 0, 1, 3).reshape(4, 8, 128)
    kept = jnp.stack(in_order(traded(kept, "y"), "y"))
    kept = kept.reshape(4, 4, 8, 32).transpose(1, 0, 2, 3).reshape(2, LAYERS, 32, 32)
    window = jnp.concatenate([later[4][:, :, 1:], kept[1].astype(bf16)[:, :, None]], axis=2)
    return second.T, kept[0], window


def solution(mesh):
    torus = Mesh(mesh.devices.reshape(8, 2, 2, 4, 4, 2), AXES)
    in_specs = (
        P(None, DP + TP),
        P(DP),
        P(None, DP, TP),
        P(None, DP, None, TP),
        P(None, DP),
        P(None, DP, TP),
        P(None, DP, TP),
        P(None, None, TP),
        P(None, None, TP),
        P(None, None, TP),
        P(None, TP),
        P(None, TP, DP),
    )
    out_specs = (P(None, DP + TP), P(None, DP, TP), P(None, DP, None, TP))
    return jax.shard_map(
        both_blocks, mesh=torus, in_specs=in_specs, out_specs=out_specs, check_vma=False
    )
```

```python
import jax
import jax.numpy as jnp
from jax import lax
from jax.sharding import Mesh
from jax.sharding import PartitionSpec as P


D = 4096
BLOCK = 256
LAYERS = 2
TAPS = 4
AXES = ("zh", "zm", "zl", "y", "x", "core")
Z = ("zh", "zm", "zl")
ZQ = ("zm", "zl")
TP = ("zh", "zm", "zl", "y")
DP = ("x", "core")
PLANE = ("x", "core", "y")
PAIRED_PLANE = ("zl", "y", "x", "core")
FIRST_GATHER = 24
FIRST_REDUCE = 4
FIRST_LAST = 20
bf16 = jnp.bfloat16
f32 = jnp.float32


epsilon = 1e-06


def exchange(tiles, axes):
    return lax.all_to_all(tiles, axes, 0, 0, tiled=True)


def exchange_far(tiles, axes, first):
    count = lax.axis_size(axes)
    order = [(first + at) % count for at in range(count)]
    return lax.all_to_all(tiles, axes, 0, 0, axis_index_groups=[order], tiled=True)


def everywhere(array, axes, first):
    count = lax.axis_size(axes)
    tiles = jnp.broadcast_to(array[None], (count, *array.shape))
    return exchange_far(tiles, axes, first)


def passed(piece, axis, flip):
    return lax.ppermute(piece, axis, [(at, at ^ flip) for at in range(lax.axis_size(axis))])


def traded(tiles, axis):
    here = lax.axis_index(axis)
    pieces = [lax.dynamic_slice_in_dim(tiles, here ^ flip, 1)[0] for flip in range(4)]
    return pieces[:1] + [passed(pieces[flip], axis, flip) for flip in range(1, 4)]


def in_order(pieces, axis):
    here = lax.axis_index(axis)
    pieces = [jnp.where((here & 1) == 1, pieces[k ^ 1], pieces[k]) for k in range(4)]
    return [jnp.where(here > 1, pieces[k ^ 2], pieces[k]) for k in range(4)]


def parts_of(value):
    coarse = lax.reduce_precision(value, 8, 7)
    rest = value - coarse
    middle = lax.reduce_precision(rest, 8, 7)
    return [coarse.astype(bf16), middle.astype(bf16), (rest - middle).astype(bf16)]


def whole_of(coarse, middle, fine):
    return coarse.astype(f32) + (middle.astype(f32) + fine.astype(f32))


def contract(a, a_dim, b, b_dim):
    return lax.dot_general(a, b, (((a_dim,), (b_dim,)), ((), ())), preferred_element_type=f32)


def grouped_features(rows_by_feature, first):
    width = rows_by_feature.shape[1]
    to = jnp.arange(width, dtype=jnp.int32)
    source = ((to % 128) // 4 + first) % 32 * 16 + to // 128 * 4 + to % 4
    chosen = (jnp.arange(width, dtype=jnp.int32)[:, None] == source[None, :]).astype(bf16)
    return contract(rows_by_feature, 1, chosen, 0).astype(bf16)


def gated_step(branch, gate_in, upper, history, taps, gates, decay, earlier):
    convolved = (
        jnp.sum(history * taps[:3, None], axis=0) + branch.astype(f32) * taps[3]
    ).astype(bf16)
    half = BLOCK // 2
    mapped = [
        contract(convolved[:, :half], 1, gates[kind, 0], 1)
        + contract(convolved[:, half:], 1, gates[kind, 1], 1)
        for kind in range(2)
    ]
    own = jnp.where(upper, convolved[:, half:], convolved[:, :half])
    input_gate = jax.nn.sigmoid(mapped[0])
    recur_gate = jax.nn.sigmoid(mapped[1])
    log_keep = 8.0 * recur_gate * decay
    keeping = jnp.exp(log_keep)
    feeding = jnp.sqrt(-jnp.expm1(2.0 * log_keep))
    state = keeping * earlier + feeding * input_gate * own.astype(f32)
    readout = (state * jax.nn.gelu(gate_in.astype(f32))).astype(bf16)
    own_branch = jnp.where(upper, branch[:, half:], branch[:, :half])
    return state, own_branch, readout


def both_blocks(
    stream,
    lengths,
    prior_state,
    prior_window,
    norm_gain,
    w_branch,
    w_gate_branch,
    conv_taps,
    w_in_gate,
    w_rec_gate,
    decay_param,
    w_out,
):
    zl = lax.axis_index("zl")
    upper = zl == 1

    stream_t = everywhere(stream.T, Z, FIRST_GATHER).reshape(128, 256)

    def scaled(weight, layer):
        return (weight[layer].T.astype(f32) * norm_gain[layer]).astype(bf16)

    def grouped(*weights):
        rows = grouped_features(jnp.concatenate(weights), FIRST_GATHER)
        return rows.reshape(-1, 4, 128).transpose(1, 0, 2)

    first_weights = grouped(scaled(w_branch, 0), scaled(w_gate_branch, 0), w_out[0])
    second_weights = grouped(scaled(w_branch, 1), scaled(w_gate_branch, 1))

    gate_rows = (
        jnp.stack([w_in_gate, w_rec_gate], axis=1)
        .reshape(LAYERS, 2, 2, 128, 32)
        .transpose(0, 1, 2, 4, 3)
        .reshape(256, 128)
    )
    depth = TAPS - 1
    needed = depth + 1 - jnp.arange(depth, dtype=jnp.int32)
    living = lengths[None, :, None, None] >= needed[None, None, :, None]
    history = jnp.where(living, prior_window, jnp.zeros_like(prior_window))
    earlier = jnp.where(
        lengths[None, :, None] >= 2, prior_state, jnp.zeros_like(prior_state)
    )

    def by_rows(groups):
        packed = jnp.concatenate(groups, axis=1).reshape(4, 8, -1, 128)
        return packed.transpose(0, 2, 1, 3).reshape(4, -1, 128)

    def for_all(rows):
        return jnp.broadcast_to(rows[None], (4, 8, 32)).reshape(32, 32)

    decay = jnp.concatenate(
        parts_of(jax.nn.log_sigmoid(decay_param)) + [jnp.zeros((2, 32), bf16)]
    )
    none = jnp.zeros((32, 32), bf16)
    small = by_rows(
        [part[layer] for layer in range(LAYERS) for part in parts_of(earlier)]
        + [for_all(decay), none]
    )
    windows = by_rows(
        [history[layer, :, tap] for layer in range(LAYERS) for tap in range(depth)]
        + [for_all(conv_taps.reshape(8, 32)), none]
    )

    def for_each(rows):
        return jnp.broadcast_to(rows.reshape(1, -1, 128), (4, rows.size // 128, 128))

    near = jnp.concatenate(
        [
            first_weights[:, :64],
            for_each(gate_rows[:128]),
            for_each(first_weights[:, 64:]),
            small,
            windows,
        ],
        axis=1,
    )
    near = jnp.stack(in_order(traded(near, "y"), "y"))
    w_first = near[:, :64].reshape(4, 2, 32, 128).transpose(1, 0, 2, 3).reshape(2, 128, 128)

    def gates_of(rows):
        return (
            rows.reshape(4, 2, 2, 32, 128).transpose(1, 2, 0, 3, 4).reshape(2, 2, 128, 128)
        )

    gates = gates_of(near[:, 64:192])

    def by_group(rows):
        rows = rows.reshape(4, -1, 8, 4, 32).transpose(1, 3, 2, 0, 4)
        return rows.reshape(-1, 8, 128)

    groups = by_group(near[:, 320:])
    shared = jnp.concatenate(
        [
            near[:, 192:320].reshape(4, 4, 32, 128).transpose(1, 0, 2, 3).reshape(4, 128, 128),
            second_weights,
            for_each(near[:, 336:]),
        ],
        axis=1,
    )
    shared = traded(shared, ZQ)
    partner = by_group(shared[1][192:].reshape(4, 16, 128))
    windows = jnp.concatenate(
        [jnp.where(upper, partner, groups[8:]), jnp.where(upper, groups[8:], partner)], axis=2
    ).astype(f32)
    shared = in_order([piece[:192] for piece in shared], ZQ)
    w_mid = jnp.concatenate([piece[:128] for piece in shared])
    later_rows = jnp.concatenate(
        [
            for_each(gate_rows[128:]),
            for_each(jnp.concatenate([piece[128:] for piece in shared])),
            grouped_features(w_out[1], FIRST_LAST).reshape(32, 4, 128).transpose(1, 0, 2),
        ],
        axis=1,
    )
    later_rows = jnp.stack(in_order(traded(later_rows, "y"), "y"))
    gates_second = gates_of(later_rows[:, :128])
    w_second = (
        later_rows[:, 128:384]
        .reshape(4, 4, 2, 32, 128)
        .transpose(1, 2, 0, 3, 4)
        .reshape(1024, 128)
    )
    w_last = later_rows[:, 384:].reshape(128, 128)

    earlier_rows = [whole_of(*groups[3 * layer : 3 * layer + 3]) for layer in range(LAYERS)]
    decay = whole_of(groups[6][:2], groups[6][2:4], groups[6][4:6])[:, None]
    history_rows = windows[:6].reshape(LAYERS, depth, 8, 256)
    taps = windows[6].reshape(LAYERS, TAPS, 256)

    products = [
        contract(stream_t, 0, w_first[kind], 1).astype(bf16).reshape(8, 4, 8, 128)
        for kind in range(2)
    ]
    products.append(stream_t.T.reshape(8, 4, 8, 128))
    branch, gate_in, rows = [part.transpose(1, 0, 2, 3) for part in products]
    sent = jnp.stack(
        [
            jnp.stack([branch, jnp.where(upper, rows, gate_in)], axis=2),
            jnp.stack([branch, jnp.where(upper, gate_in, rows)], axis=2),
        ]
    )
    came = exchange(sent.reshape(64, 16, 128), PAIRED_PLANE)
    came = came.reshape(2, 32, 2, 8, 128)
    later = (history_rows[1], taps[1], decay[1], earlier_rows[1], history)
    branch = came[:, :, 0].astype(f32).sum(axis=1)
    branch = jnp.concatenate([branch[0], branch[1]], axis=1)
    rows = jnp.where(upper, came[0, :, 1], came[1, :, 1])
    gate_in = jnp.where(upper, came[1, :, 1], came[0, :, 1]).astype(f32).sum(axis=0)
    widened = rows.astype(f32)
    squares = jnp.sum(jnp.sum(widened * widened, axis=0), axis=1, keepdims=True)
    scaling = lax.rsqrt(squares / D + epsilon)
    state_first, branch_first, readout = gated_step(
        (branch * scaling).astype(bf16),
        (gate_in * scaling).astype(bf16),
        upper,
        history_rows[0],
        taps[0],
        gates,
        decay[0],
        earlier_rows[0],
    )
    sent = jnp.stack([jnp.broadcast_to(readout[None], (32, 8, 128)), rows], axis=1)
    came = exchange(sent.reshape(32, 16, 128), ZQ + DP).reshape(4, 8, 2, 8, 128)
    residual = came[0, :, 1].reshape(64, 128).astype(f32)
    came = came[:, :, 0].reshape(4, 64, 128)
    came = jnp.concatenate([came[at] for at in range(4)], axis=1)
    mixed = contract(came, 1, w_mid, 0).astype(bf16)
    mixed = everywhere(mixed, "zh", FIRST_REDUCE)
    mixed, w_second, gates_second, w_last = lax.optimization_barrier(
        (mixed, w_second, gates_second, w_last)
    )
    mixed = mixed.astype(f32).sum(axis=0)
    first = (mixed + residual).astype(bf16)

    products = contract(first, 1, w_second, 1).astype(bf16)
    products = [products[:, 128 * at : 128 * (at + 1)].reshape(8, 8, 128) for at in range(8)]
    own_rows = first.reshape(8, 8, 128)
    sent = jnp.stack(
        [
            jnp.stack(
                [
                    products[4 * zm],
                    products[4 * zm + 2],
                    products[4 * zm + 2 * low + 1],
                    own_rows,
                ],
                axis=1,
            )
            for zm in range(2)
            for low in range(2)
        ]
    )
    came = exchange(sent.reshape(32, 32, 128), ZQ + DP).reshape(32, 4, 8, 128)
    rows = came[:, 3]
    came = came[:, :3].astype(f32).sum(axis=0)
    widened = rows.astype(f32)
    squares = jnp.sum(jnp.sum(widened * widened, axis=0), axis=1, keepdims=True)
    branch = jnp.concatenate([came[0], came[1]], axis=1)
    scaling = lax.rsqrt(squares / D + epsilon)
    state_second, branch_second, readout = gated_step(
        (branch * scaling).astype(bf16),
        (came[2] * scaling).astype(bf16),
        upper,
        later[0],
        later[1],
        gates_second,
        later[2],
        later[3],
    )
    sent = jnp.stack(
        [
            jnp.broadcast_to(readout[None], (32, 8, 128)),
            rows.reshape(4, 8, 8, 128).transpose(1, 0, 2, 3).reshape(32, 8, 128),
        ],
        axis=1,
    )
    came = exchange(sent.reshape(32, 16, 128), PLANE).reshape(32, 2, 8, 128)
    mixed = contract(w_last, 0, came[:, 0].reshape(256, 128), 1).astype(bf16)
    mixed = mixed.reshape(32, 4, 256)
    own = (lax.axis_index(Z) - FIRST_GATHER) % 32 * 4
    own = lax.broadcasted_iota(jnp.int32, (4, 128), 0) + own
    own = (own == lax.broadcasted_iota(jnp.int32, (4, 128), 1)).astype(bf16)
    residual = contract(own, 1, came[:, 1].reshape(256, 128), 1)
    second = exchange_far(mixed, Z, FIRST_LAST).astype(f32).sum(axis=0)
    second = (second + residual).astype(bf16)

    kept = jnp.stack(
        [state_first, state_second, branch_first.astype(f32), branch_second.astype(f32)]
    )
    kept = kept.reshape(4, 8, 4, 32).transpose(2, 0, 1, 3).reshape(4, 8, 128)
    kept = jnp.stack(in_order(traded(kept, "y"), "y"))
    kept = kept.reshape(4, 4, 8, 32).transpose(1, 0, 2, 3).reshape(2, LAYERS, 32, 32)
    window = jnp.concatenate([later[4][:, :, 1:], kept[1].astype(bf16)[:, :, None]], axis=2)
    return second.T, kept[0], window


def solution(mesh):
    torus = Mesh(mesh.devices.reshape(8, 2, 2, 4, 4, 2), AXES)
    in_specs = (
        P(None, DP + TP),
        P(DP),
        P(None, DP, TP),
        P(None, DP, None, TP),
        P(None, DP),
        P(None, DP, TP),
        P(None, DP, TP),
        P(None, None, TP),
        P(None, None, TP),
        P(None, None, TP),
        P(None, TP),
        P(None, TP, DP),
    )
    out_specs = (P(None, DP + TP), P(None, DP, TP), P(None, DP, None, TP))
    return jax.shard_map(
        both_blocks, mesh=torus, in_specs=in_specs, out_specs=out_specs, check_vma=False
    )
```

```python
import jax
import jax.numpy as jnp
from jax import lax
from jax.experimental import pallas as pl
from jax.experimental.pallas import tpu as pltpu
from jax.sharding import Mesh
from jax.sharding import PartitionSpec as P


D = 4096
BLOCK = 256
LAYERS = 2
TAPS = 4
AXES = ("zh", "zm", "zl", "y", "x", "core")
Z = ("zh", "zm", "zl")
ZQ = ("zm", "zl")
TP = ("zh", "zm", "zl", "y")
DP = ("x", "core")
PLANE = ("x", "core", "y")
PAIRED_PLANE = ("zl", "y", "x", "core")
FIRST_GATHER = 24
FIRST_REDUCE = 4
FIRST_LAST = 20
bf16 = jnp.bfloat16
f32 = jnp.float32


epsilon = 1e-06


def exchange(tiles, axes):
    return lax.all_to_all(tiles, axes, 0, 0, tiled=True)


def exchange_far(tiles, axes, first):
    count = lax.axis_size(axes)
    order = [(first + at) % count for at in range(count)]
    return lax.all_to_all(tiles, axes, 0, 0, axis_index_groups=[order], tiled=True)


def everywhere(array, axes, first):
    count = lax.axis_size(axes)
    tiles = jnp.broadcast_to(array[None], (count, *array.shape))
    return exchange_far(tiles, axes, first)


def passed(piece, axis, flip):
    return lax.ppermute(piece, axis, [(at, at ^ flip) for at in range(lax.axis_size(axis))])


def traded(tiles, axis):
    here = lax.axis_index(axis)
    tiles = tiles if isinstance(tiles, list) else [tiles] * 4
    pieces = [lax.dynamic_slice_in_dim(tiles[flip], here ^ flip, 1)[0] for flip in range(4)]
    return pieces[:1] + [passed(pieces[flip], axis, flip) for flip in range(1, 4)]


def in_order(pieces, axis):
    here = lax.axis_index(axis)
    pieces = [jnp.where((here & 1) == 1, pieces[k ^ 1], pieces[k]) for k in range(4)]
    return [jnp.where(here > 1, pieces[k ^ 2], pieces[k]) for k in range(4)]


def whole_of(coarse, middle, fine):
    return coarse.astype(f32) + (middle.astype(f32) + fine.astype(f32))


def contract(a, a_dim, b, b_dim):
    return lax.dot_general(a, b, (((a_dim,), (b_dim,)), ((), ())), preferred_element_type=f32)


def grouped_features(rows_by_feature, first):
    width = rows_by_feature.shape[1]
    to = jnp.arange(width, dtype=jnp.int32)
    source = ((to % 128) // 4 + first) % 32 * 16 + to // 128 * 4 + to % 4
    chosen = (jnp.arange(width, dtype=jnp.int32)[:, None] == source[None, :]).astype(bf16)
    return contract(rows_by_feature, 1, chosen, 0).astype(bf16)


def pack_kernel(branch, gate, out, in_gate, rec_gate, gain, state, window, taps, decay, packed, later):
    row = lax.broadcasted_iota(jnp.int32, (8, 32), 0)
    weights = [
        (weight[layer].astype(f32) * gain[layer : layer + 1]).astype(bf16)
        for layer in range(2)
        for weight in (branch, gate)
    ]
    width = 512
    to = lax.broadcasted_iota(jnp.int32, (width, width), 1)
    source = (((to & 127) >> 2) + FIRST_GATHER & 31) * 16 + (to >> 7) * 4 + (to & 3)
    chosen = lax.broadcasted_iota(jnp.int32, (width, width), 0) == source
    chosen = jnp.where(chosen, 1.0, 0.0).astype(bf16)
    weights = jnp.concatenate([*weights, out[0]], axis=0)
    weights = jnp.dot(weights, chosen, preferred_element_type=f32).astype(bf16)

    def split(value):
        coarse = value.astype(bf16).astype(f32)
        middle = (value - coarse).astype(bf16).astype(f32)
        return [coarse, middle, value - coarse - middle]

    rates = split(jnp.where((row & 1) == 0, decay[:1], decay[1:2]))
    rates = jnp.where(row < 2, rates[0], jnp.where(row < 4, rates[1], rates[2]))
    rates = jnp.where(row < 6, rates, 0.0)
    tap_rows = jnp.concatenate([taps[0].astype(f32), taps[1].astype(f32)], axis=0)
    none = jnp.zeros((32, 32), f32)
    small = [part for layer in range(2) for part in split(state[layer])]
    small = small + [jnp.concatenate([rates] * 4, axis=0), none]
    small = small + [window[layer, tap].astype(f32) for layer in range(2) for tap in range(3)]
    small = small + [jnp.concatenate([tap_rows] * 4, axis=0), none]
    small = [jnp.concatenate(small[4 * at : 4 * at + 4], axis=1) for at in range(4)]
    for y in range(4):
        packed[y, :64] = weights[:64, 128 * y : 128 * (y + 1)]
        for kind, weight in enumerate((in_gate, rec_gate)):
            for half in range(2):
                place = 64 + 32 * (2 * kind + half)
                packed[y, place : place + 32] = weight[0, :, 128 * half : 128 * (half + 1)]
        for q in range(4):
            place = 192 + 32 * q
            packed[y, place : place + 32] = weights[128:, 128 * q : 128 * (q + 1)]
        later[y] = weights[64:128, 128 * y : 128 * (y + 1)]
        for at in range(4):
            place = 320 + 8 * at
            packed[y, place : place + 8] = small[at][8 * y : 8 * (y + 1)].astype(bf16)


def packed_for_y(*arrays):
    return pl.pallas_call(
        pack_kernel,
        out_shape=[
            jax.ShapeDtypeStruct((4, 352, 128), bf16),
            jax.ShapeDtypeStruct((4, 64, 128), bf16),
        ],
        compiler_params=pltpu.CompilerParams(vmem_limit_bytes=8 * 2**20),
        cost_estimate=pl.CostEstimate(flops=100_000_000, bytes_accessed=800_000, transcendentals=0),
    )(*arrays)


def gated_step(branch, gate_in, upper, history, taps, gates, decay, earlier):
    convolved = (
        jnp.sum(history * taps[:3, None], axis=0) + branch.astype(f32) * taps[3]
    ).astype(bf16)
    half = BLOCK // 2
    mapped = [
        contract(convolved[:, :half], 1, gates[kind, 0], 1)
        + contract(convolved[:, half:], 1, gates[kind, 1], 1)
        for kind in range(2)
    ]
    own = jnp.where(upper, convolved[:, half:], convolved[:, :half])
    input_gate = jax.nn.sigmoid(mapped[0])
    recur_gate = jax.nn.sigmoid(mapped[1])
    log_keep = 8.0 * recur_gate * decay
    keeping = jnp.exp(log_keep)
    feeding = jnp.sqrt(-jnp.expm1(2.0 * log_keep))
    state = keeping * earlier + feeding * input_gate * own.astype(f32)
    readout = (state * jax.nn.gelu(gate_in.astype(f32))).astype(bf16)
    own_branch = jnp.where(upper, branch[:, half:], branch[:, :half])
    return state, own_branch, readout


def both_blocks(
    stream,
    lengths,
    prior_state,
    prior_window,
    norm_gain,
    w_branch,
    w_gate_branch,
    conv_taps,
    w_in_gate,
    w_rec_gate,
    decay_param,
    w_out,
):
    zl = lax.axis_index("zl")
    upper = zl == 1

    stream_t = everywhere(stream.T, Z, FIRST_GATHER).reshape(128, 256)

    second_gate_rows = jnp.concatenate(
        [
            weight[1, 128 * half : 128 * (half + 1)].T
            for weight in (w_in_gate, w_rec_gate)
            for half in range(2)
        ]
    )
    depth = TAPS - 1

    def for_each(rows):
        return jnp.broadcast_to(rows.reshape(1, -1, 128), (4, rows.size // 128, 128))

    near, second_weights = packed_for_y(
        w_branch.transpose(0, 2, 1),
        w_gate_branch.transpose(0, 2, 1),
        w_out,
        w_in_gate.transpose(0, 2, 1),
        w_rec_gate.transpose(0, 2, 1),
        norm_gain,
        prior_state,
        prior_window.transpose(0, 2, 1, 3),
        conv_taps,
        decay_param,
    )
    near = jnp.stack(in_order(traded(near, "y"), "y"))
    w_first = near[:, :64].reshape(4, 2, 32, 128).transpose(1, 0, 2, 3).reshape(2, 128, 128)
    index = lax.broadcasted_iota(jnp.int32, (128, 128), 0)
    same = (index == lax.broadcasted_iota(jnp.int32, (128, 128), 1)).astype(bf16)
    w_first = jnp.concatenate(
        [w_first[0], jnp.where(upper, same, w_first[1]), jnp.where(upper, w_first[1], same)]
    )

    def gates_of(rows):
        return (
            rows.reshape(4, 2, 2, 32, 128).transpose(1, 2, 0, 3, 4).reshape(2, 2, 128, 128)
        )

    gates = gates_of(near[:, 64:192])

    def by_group(rows):
        rows = rows.reshape(4, -1, 8, 4, 32).transpose(1, 3, 2, 0, 4)
        return rows.reshape(-1, 8, 128)

    groups = by_group(near[:, 320:])
    shared = jnp.concatenate(
        [
            near[:, 192:320].reshape(4, 4, 32, 128).transpose(1, 0, 2, 3).reshape(4, 128, 128),
            second_weights,
        ],
        axis=1,
    )
    with_windows = jnp.concatenate([shared, for_each(near[:, 336:])], axis=1)
    shared = traded([shared, with_windows, shared, shared], ZQ)
    partner = by_group(shared[1][192:].reshape(4, 16, 128))
    windows = jnp.concatenate(
        [jnp.where(upper, partner, groups[8:]), jnp.where(upper, groups[8:], partner)], axis=2
    ).astype(f32)
    shared = in_order([piece[:192] for piece in shared], ZQ)
    w_mid = jnp.concatenate([piece[:128] for piece in shared])
    later_rows = jnp.concatenate(
        [
            for_each(second_gate_rows),
            for_each(jnp.concatenate([piece[128:] for piece in shared])),
            grouped_features(w_out[1], FIRST_LAST).reshape(32, 4, 128).transpose(1, 0, 2),
        ],
        axis=1,
    )
    later_rows = jnp.stack(in_order(traded(later_rows, "y"), "y"))
    gates_second = gates_of(later_rows[:, :128])
    w_second = (
        later_rows[:, 128:384]
        .reshape(4, 4, 2, 32, 128)
        .transpose(1, 2, 0, 3, 4)
        .reshape(1024, 128)
    )
    w_last = later_rows[:, 384:].reshape(128, 128)

    own_lengths = lax.dynamic_slice_in_dim(lengths, lax.axis_index("y") * 8, 8)[:, None]
    earlier_rows = [
        jnp.where(own_lengths >= 2, whole_of(*groups[3 * layer : 3 * layer + 3]), 0.0)
        for layer in range(LAYERS)
    ]
    decay = whole_of(groups[6][:2], groups[6][2:4], groups[6][4:6])[:, None]
    decay = jax.nn.log_sigmoid(decay)
    needed = depth + 1 - jnp.arange(depth, dtype=jnp.int32)
    history_rows = jnp.where(
        own_lengths >= needed[:, None, None], windows[:6].reshape(LAYERS, depth, 8, 256), 0.0
    )
    taps = windows[6].reshape(LAYERS, TAPS, 256)

    products = contract(stream_t, 0, w_first, 1).astype(bf16)
    products = products.reshape(8, 4, 8, 3, 128).transpose(3, 1, 0, 2, 4)
    sent = jnp.stack(
        [
            jnp.stack([products[0], products[1]], axis=2),
            jnp.stack([products[0], products[2]], axis=2),
        ]
    )
    came = exchange(sent.reshape(64, 16, 128), PAIRED_PLANE)
    came = came.reshape(2, 32, 2, 8, 128)
    later = (history_rows[1], taps[1], decay[1], earlier_rows[1])
    branch = came[:, :, 0].astype(f32).sum(axis=1)
    branch = jnp.concatenate([branch[0], branch[1]], axis=1)
    rows = jnp.where(upper, came[0, :, 1], came[1, :, 1])
    gate_in = jnp.where(upper, came[1, :, 1], came[0, :, 1]).astype(f32).sum(axis=0)
    widened = rows.astype(f32)
    squares = jnp.sum(jnp.sum(widened * widened, axis=0), axis=1, keepdims=True)
    scaling = lax.rsqrt(squares / D + epsilon)
    state_first, branch_first, readout = gated_step(
        (branch * scaling).astype(bf16),
        (gate_in * scaling).astype(bf16),
        upper,
        history_rows[0],
        taps[0],
        gates,
        decay[0],
        earlier_rows[0],
    )
    sent = jnp.stack([jnp.broadcast_to(readout[None], (32, 8, 128)), rows], axis=1)
    came = exchange(sent.reshape(32, 16, 128), ZQ + DP).reshape(4, 8, 2, 8, 128)
    residual = came[0, :, 1].reshape(64, 128).astype(f32)
    came = came[:, :, 0].reshape(4, 64, 128)
    came = jnp.concatenate([came[at] for at in range(4)], axis=1)
    mixed = contract(came, 1, w_mid, 0).astype(bf16)
    mixed = everywhere(mixed, "zh", FIRST_REDUCE)
    mixed, w_second, gates_second, w_last = lax.optimization_barrier(
        (mixed, w_second, gates_second, w_last)
    )
    mixed = mixed.astype(f32).sum(axis=0)
    first = (mixed + residual).astype(bf16)

    products = contract(first, 1, w_second, 1).astype(bf16)
    products = [products[:, 128 * at : 128 * (at + 1)].reshape(8, 8, 128) for at in range(8)]
    own_rows = first.reshape(8, 8, 128)
    sent = jnp.stack(
        [
            jnp.stack(
                [
                    products[4 * zm],
                    products[4 * zm + 2],
                    products[4 * zm + 2 * low + 1],
                    own_rows,
                ],
                axis=1,
            )
            for zm in range(2)
            for low in range(2)
        ]
    )
    came = exchange(sent.reshape(32, 32, 128), ZQ + DP).reshape(32, 4, 8, 128)
    came, state_first, branch_first = lax.optimization_barrier((came, state_first, branch_first))
    rows = came[:, 3]
    came = came[:, :3].astype(f32).sum(axis=0)
    widened = rows.astype(f32)
    squares = jnp.sum(jnp.sum(widened * widened, axis=0), axis=1, keepdims=True)
    branch = jnp.concatenate([came[0], came[1]], axis=1)
    scaling = lax.rsqrt(squares / D + epsilon)
    state_second, branch_second, readout = gated_step(
        (branch * scaling).astype(bf16),
        (came[2] * scaling).astype(bf16),
        upper,
        later[0],
        later[1],
        gates_second,
        later[2],
        later[3],
    )
    sent = jnp.stack(
        [
            jnp.broadcast_to(readout[None], (32, 8, 128)),
            rows.reshape(4, 8, 8, 128).transpose(1, 0, 2, 3).reshape(32, 8, 128),
        ],
        axis=1,
    )
    came = exchange(sent.reshape(32, 16, 128), PLANE).reshape(32, 2, 8, 128)
    mixed = contract(w_last, 0, came[:, 0].reshape(256, 128), 1).astype(bf16)
    mixed = mixed.reshape(32, 4, 256)
    own = (lax.axis_index(Z) - FIRST_GATHER) % 32 * 4
    own = lax.broadcasted_iota(jnp.int32, (4, 128), 0) + own
    own = (own == lax.broadcasted_iota(jnp.int32, (4, 128), 1)).astype(bf16)
    residual = contract(own, 1, came[:, 1].reshape(256, 128), 1)
    second = exchange_far(mixed, Z, FIRST_LAST).astype(f32).sum(axis=0)
    second = (second + residual).astype(bf16)

    kept = jnp.stack(
        [state_first, state_second, branch_first.astype(f32), branch_second.astype(f32)]
    )
    kept = kept.reshape(4, 8, 4, 32).transpose(2, 0, 1, 3).reshape(4, 8, 128)
    kept = jnp.stack(in_order(traded(kept, "y"), "y"))
    kept = kept.reshape(4, 4, 8, 32).transpose(1, 0, 2, 3).reshape(2, LAYERS, 32, 32)
    living = lengths[None, :, None, None] >= needed[None, None, 1:, None]
    history = jnp.where(living, prior_window[:, :, 1:], jnp.zeros_like(prior_window[:, :, 1:]))
    window = jnp.concatenate([history, kept[1].astype(bf16)[:, :, None]], axis=2)
    return second.T, kept[0], window


def solution(mesh):
    torus = Mesh(mesh.devices.reshape(8, 2, 2, 4, 4, 2), AXES)
    in_specs = (
        P(None, DP + TP),
        P(DP),
        P(None, DP, TP),
        P(None, DP, None, TP),
        P(None, DP),
        P(None, DP, TP),
        P(None, DP, TP),
        P(None, None, TP),
        P(None, None, TP),
        P(None, None, TP),
        P(None, TP),
        P(None, TP, DP),
    )
    out_specs = (P(None, DP + TP), P(None, DP, TP), P(None, DP, None, TP))
    return jax.shard_map(
        both_blocks, mesh=torus, in_specs=in_specs, out_specs=out_specs, check_vma=False
    )
```

```python
import jax
import jax.numpy as jnp
from jax import lax
from jax.experimental import pallas as pl
from jax.experimental.pallas import tpu as pltpu
from jax.sharding import Mesh
from jax.sharding import PartitionSpec as P


D = 4096
BLOCK = 256
LAYERS = 2
TAPS = 4
AXES = ("zh", "zm", "zl", "y", "x", "core")
Z = ("zh", "zm", "zl")
ZQ = ("zm", "zl")
TP = ("zh", "zm", "zl", "y")
DP = ("x", "core")
PLANE = ("x", "core", "y")
PAIRED_PLANE = ("zl", "y", "x", "core")
FIRST_GATHER = 22
FIRST_REDUCE = 3
FIRST_LAST = 18
bf16 = jnp.bfloat16
f32 = jnp.float32


epsilon = 1e-06


def exchange(tiles, axes):
    return lax.all_to_all(tiles, axes, 0, 0, tiled=True)


def exchange_far(tiles, axes, first):
    count = lax.axis_size(axes)
    order = [(first + at) % count for at in range(count)]
    return lax.all_to_all(tiles, axes, 0, 0, axis_index_groups=[order], tiled=True)


def everywhere(array, axes, first):
    count = lax.axis_size(axes)
    tiles = jnp.broadcast_to(array[None], (count, *array.shape))
    return exchange_far(tiles, axes, first)


def passed(piece, axis, flip):
    return lax.ppermute(piece, axis, [(at, at ^ flip) for at in range(lax.axis_size(axis))])


def traded(tiles, axis):
    here = lax.axis_index(axis)
    tiles = tiles if isinstance(tiles, list) else [tiles] * 4
    pieces = [lax.dynamic_slice_in_dim(tiles[flip], here ^ flip, 1)[0] for flip in range(4)]
    return pieces[:1] + [passed(pieces[flip], axis, flip) for flip in range(1, 4)]


def in_order(pieces, axis):
    here = lax.axis_index(axis)
    pieces = [jnp.where((here & 1) == 1, pieces[k ^ 1], pieces[k]) for k in range(4)]
    return [jnp.where(here > 1, pieces[k ^ 2], pieces[k]) for k in range(4)]


def whole_of(coarse, middle, fine):
    return coarse.astype(f32) + (middle.astype(f32) + fine.astype(f32))


def contract(a, a_dim, b, b_dim):
    return lax.dot_general(a, b, (((a_dim,), (b_dim,)), ((), ())), preferred_element_type=f32)


def grouped_features(rows_by_feature, first):
    width = rows_by_feature.shape[1]
    to = jnp.arange(width, dtype=jnp.int32)
    source = ((to % 128) // 4 + first) % 32 * 16 + to // 128 * 4 + to % 4
    chosen = (jnp.arange(width, dtype=jnp.int32)[:, None] == source[None, :]).astype(bf16)
    return contract(rows_by_feature, 1, chosen, 0).astype(bf16)


def pack_kernel(branch, gate, out, in_gate, rec_gate, gain, state, window, taps, decay, packed, later):
    row = lax.broadcasted_iota(jnp.int32, (8, 32), 0)
    weights = [
        (weight[layer].astype(f32) * gain[layer : layer + 1]).astype(bf16)
        for layer in range(2)
        for weight in (branch, gate)
    ]
    width = 512
    to = lax.broadcasted_iota(jnp.int32, (width, width), 1)
    source = (((to & 127) >> 2) + FIRST_GATHER & 31) * 16 + (to >> 7) * 4 + (to & 3)
    chosen = lax.broadcasted_iota(jnp.int32, (width, width), 0) == source
    chosen = jnp.where(chosen, 1.0, 0.0).astype(bf16)
    weights = jnp.concatenate([*weights, out[0]], axis=0)
    weights = jnp.dot(weights, chosen, preferred_element_type=f32).astype(bf16)

    def split(value):
        coarse = value.astype(bf16).astype(f32)
        middle = (value - coarse).astype(bf16).astype(f32)
        return [coarse, middle, value - coarse - middle]

    rates = split(jnp.where((row & 1) == 0, decay[:1], decay[1:2]))
    rates = jnp.where(row < 2, rates[0], jnp.where(row < 4, rates[1], rates[2]))
    rates = jnp.where(row < 6, rates, 0.0)
    tap_rows = jnp.concatenate([taps[0].astype(f32), taps[1].astype(f32)], axis=0)
    none = jnp.zeros((32, 32), f32)
    small = [part for layer in range(2) for part in split(state[layer])]
    small = small + [jnp.concatenate([rates] * 4, axis=0), none]
    small = small + [window[layer, tap].astype(f32) for layer in range(2) for tap in range(3)]
    small = small + [jnp.concatenate([tap_rows] * 4, axis=0), none]
    small = [jnp.concatenate(small[4 * at : 4 * at + 4], axis=1) for at in range(4)]
    for y in range(4):
        packed[y, :64] = weights[:64, 128 * y : 128 * (y + 1)]
        for kind, weight in enumerate((in_gate, rec_gate)):
            for half in range(2):
                place = 64 + 32 * (2 * kind + half)
                packed[y, place : place + 32] = weight[0, :, 128 * half : 128 * (half + 1)]
        for q in range(4):
            place = 192 + 32 * q
            packed[y, place : place + 32] = weights[128:, 128 * q : 128 * (q + 1)]
        later[y] = weights[64:128, 128 * y : 128 * (y + 1)]
        for at in range(4):
            place = 320 + 8 * at
            packed[y, place : place + 8] = small[at][8 * y : 8 * (y + 1)].astype(bf16)


def packed_for_y(*arrays):
    return pl.pallas_call(
        pack_kernel,
        out_shape=[
            jax.ShapeDtypeStruct((4, 352, 128), bf16),
            jax.ShapeDtypeStruct((4, 64, 128), bf16),
        ],
        compiler_params=pltpu.CompilerParams(vmem_limit_bytes=8 * 2**20),
        cost_estimate=pl.CostEstimate(flops=100_000_000, bytes_accessed=800_000, transcendentals=0),
    )(*arrays)


def gated_step(branch, gate_in, upper, history, taps, gates, decay, earlier):
    convolved = (
        jnp.sum(history * taps[:3, None], axis=0) + branch.astype(f32) * taps[3]
    ).astype(bf16)
    half = BLOCK // 2
    mapped = [
        contract(convolved[:, :half], 1, gates[kind, 0], 1)
        + contract(convolved[:, half:], 1, gates[kind, 1], 1)
        for kind in range(2)
    ]
    own = jnp.where(upper, convolved[:, half:], convolved[:, :half])
    input_gate = jax.nn.sigmoid(mapped[0])
    recur_gate = jax.nn.sigmoid(mapped[1])
    log_keep = 8.0 * recur_gate * decay
    keeping = jnp.exp(log_keep)
    feeding = jnp.sqrt(-jnp.expm1(2.0 * log_keep))
    state = keeping * earlier + feeding * input_gate * own.astype(f32)
    readout = (state * jax.nn.gelu(gate_in.astype(f32))).astype(bf16)
    own_branch = jnp.where(upper, branch[:, half:], branch[:, :half])
    return state, own_branch, readout


def both_blocks(
    stream,
    lengths,
    prior_state,
    prior_window,
    norm_gain,
    w_branch,
    w_gate_branch,
    conv_taps,
    w_in_gate,
    w_rec_gate,
    decay_param,
    w_out,
):
    zl = lax.axis_index("zl")
    upper = zl == 1

    stream_t = everywhere(stream.T, Z, FIRST_GATHER).reshape(128, 256)

    second_gate_rows = jnp.concatenate(
        [
            weight[1, 128 * half : 128 * (half + 1)].T
            for weight in (w_in_gate, w_rec_gate)
            for half in range(2)
        ]
    )
    depth = TAPS - 1

    def for_each(rows):
        return jnp.broadcast_to(rows.reshape(1, -1, 128), (4, rows.size // 128, 128))

    near, second_weights = packed_for_y(
        w_branch.transpose(0, 2, 1),
        w_gate_branch.transpose(0, 2, 1),
        w_out,
        w_in_gate.transpose(0, 2, 1),
        w_rec_gate.transpose(0, 2, 1),
        norm_gain,
        prior_state,
        prior_window.transpose(0, 2, 1, 3),
        conv_taps,
        decay_param,
    )
    near = jnp.stack(in_order(traded(near, "y"), "y"))
    w_first = near[:, :64].reshape(4, 2, 32, 128).transpose(1, 0, 2, 3).reshape(2, 128, 128)
    index = lax.broadcasted_iota(jnp.int32, (128, 128), 0)
    same = (index == lax.broadcasted_iota(jnp.int32, (128, 128), 1)).astype(bf16)
    w_first = jnp.concatenate(
        [w_first[0], jnp.where(upper, same, w_first[1]), jnp.where(upper, w_first[1], same)]
    )

    def gates_of(rows):
        return (
            rows.reshape(4, 2, 2, 32, 128).transpose(1, 2, 0, 3, 4).reshape(2, 2, 128, 128)
        )

    gates = gates_of(near[:, 64:192])

    def by_group(rows):
        rows = rows.reshape(4, -1, 8, 4, 32).transpose(1, 3, 2, 0, 4)
        return rows.reshape(-1, 8, 128)

    groups = by_group(near[:, 320:])
    shared = jnp.concatenate(
        [
            near[:, 192:320].reshape(4, 4, 32, 128).transpose(1, 0, 2, 3).reshape(4, 128, 128),
            second_weights,
        ],
        axis=1,
    )
    with_windows = jnp.concatenate([shared, for_each(near[:, 336:])], axis=1)
    shared = traded([shared, with_windows, shared, shared], ZQ)
    partner = by_group(shared[1][192:].reshape(4, 16, 128))
    windows = jnp.concatenate(
        [jnp.where(upper, partner, groups[8:]), jnp.where(upper, groups[8:], partner)], axis=2
    ).astype(f32)
    shared = in_order([piece[:192] for piece in shared], ZQ)
    w_mid = jnp.concatenate([piece[:128] for piece in shared])
    later_rows = jnp.concatenate(
        [
            for_each(second_gate_rows),
            for_each(jnp.concatenate([piece[128:] for piece in shared])),
            grouped_features(w_out[1], FIRST_LAST).reshape(32, 4, 128).transpose(1, 0, 2),
        ],
        axis=1,
    )
    later_rows = jnp.stack(in_order(traded(later_rows, "y"), "y"))
    gates_second = gates_of(later_rows[:, :128])
    w_second = (
        later_rows[:, 128:384]
        .reshape(4, 4, 2, 32, 128)
        .transpose(1, 2, 0, 3, 4)
        .reshape(1024, 128)
    )
    w_last = later_rows[:, 384:].reshape(128, 128)

    own_lengths = lax.dynamic_slice_in_dim(lengths, lax.axis_index("y") * 8, 8)[:, None]
    earlier_rows = [
        jnp.where(own_lengths >= 2, whole_of(*groups[3 * layer : 3 * layer + 3]), 0.0)
        for layer in range(LAYERS)
    ]
    decay = whole_of(groups[6][:2], groups[6][2:4], groups[6][4:6])[:, None]
    decay = jax.nn.log_sigmoid(decay)
    needed = depth + 1 - jnp.arange(depth, dtype=jnp.int32)
    history_rows = jnp.where(
        own_lengths >= needed[:, None, None], windows[:6].reshape(LAYERS, depth, 8, 256), 0.0
    )
    taps = windows[6].reshape(LAYERS, TAPS, 256)

    products = contract(stream_t, 0, w_first, 1).astype(bf16)
    products = products.reshape(8, 4, 8, 3, 128).transpose(3, 1, 0, 2, 4)
    sent = jnp.stack(
        [
            jnp.stack([products[0], products[1]], axis=2),
            jnp.stack([products[0], products[2]], axis=2),
        ]
    )
    came = exchange(sent.reshape(64, 16, 128), PAIRED_PLANE)
    came = came.reshape(2, 32, 2, 8, 128)
    later = (history_rows[1], taps[1], decay[1], earlier_rows[1])
    branch = came[:, :, 0].astype(f32).sum(axis=1)
    branch = jnp.concatenate([branch[0], branch[1]], axis=1)
    rows = jnp.where(upper, came[0, :, 1], came[1, :, 1])
    gate_in = jnp.where(upper, came[1, :, 1], came[0, :, 1]).astype(f32).sum(axis=0)
    widened = rows.astype(f32)
    squares = jnp.sum(jnp.sum(widened * widened, axis=0), axis=1, keepdims=True)
    scaling = lax.rsqrt(squares / D + epsilon)
    state_first, branch_first, readout = gated_step(
        (branch * scaling).astype(bf16),
        (gate_in * scaling).astype(bf16),
        upper,
        history_rows[0],
        taps[0],
        gates,
        decay[0],
        earlier_rows[0],
    )
    sent = jnp.stack([jnp.broadcast_to(readout[None], (32, 8, 128)), rows], axis=1)
    came = exchange(sent.reshape(32, 16, 128), ZQ + DP).reshape(4, 8, 2, 8, 128)
    residual = came[0, :, 1].reshape(64, 128).astype(f32)
    came = came[:, :, 0].reshape(4, 64, 128)
    came = jnp.concatenate([came[at] for at in range(4)], axis=1)
    mixed = contract(came, 1, w_mid, 0).astype(bf16)
    mixed = everywhere(mixed, "zh", FIRST_REDUCE)
    at_z = lax.axis_index(Z)
    mixed, w_second, gates_second, w_last, state_first, branch_first, at_z = (
        lax.optimization_barrier(
            (mixed, w_second, gates_second, w_last, state_first, branch_first, at_z)
        )
    )
    mixed = mixed.astype(f32).sum(axis=0)
    first = (mixed + residual).astype(bf16)

    products = contract(first, 1, w_second, 1).astype(bf16)
    products = [products[:, 128 * at : 128 * (at + 1)].reshape(8, 8, 128) for at in range(8)]
    own_rows = first.reshape(8, 8, 128)
    sent = jnp.stack(
        [
            jnp.stack(
                [
                    products[4 * zm],
                    products[4 * zm + 2],
                    products[4 * zm + 2 * low + 1],
                    own_rows,
                ],
                axis=1,
            )
            for zm in range(2)
            for low in range(2)
        ]
    )
    came = exchange(sent.reshape(32, 32, 128), ZQ + DP).reshape(32, 4, 8, 128)
    came, state_first, branch_first = lax.optimization_barrier((came, state_first, branch_first))
    rows = came[:, 3]
    came = came[:, :3].astype(f32).sum(axis=0)
    widened = rows.astype(f32)
    squares = jnp.sum(jnp.sum(widened * widened, axis=0), axis=1, keepdims=True)
    branch = jnp.concatenate([came[0], came[1]], axis=1)
    scaling = lax.rsqrt(squares / D + epsilon)
    state_second, branch_second, readout = gated_step(
        (branch * scaling).astype(bf16),
        (came[2] * scaling).astype(bf16),
        upper,
        later[0],
        later[1],
        gates_second,
        later[2],
        later[3],
    )
    sent = jnp.stack(
        [
            jnp.broadcast_to(readout[None], (32, 8, 128)),
            rows.reshape(4, 8, 8, 128).transpose(1, 0, 2, 3).reshape(32, 8, 128),
        ],
        axis=1,
    )
    came = exchange(sent.reshape(32, 16, 128), PLANE).reshape(32, 2, 8, 128)
    came, lengths, prior_window, at_z = lax.optimization_barrier(
        (came, lengths, prior_window, at_z)
    )
    mixed = contract(w_last, 0, came[:, 0].reshape(256, 128), 1).astype(bf16)
    mixed = mixed.reshape(32, 4, 256)
    own = (at_z + (32 - FIRST_GATHER) & 31) * 4
    own = lax.broadcasted_iota(jnp.int32, (4, 128), 0) + own
    own = (own == lax.broadcasted_iota(jnp.int32, (4, 128), 1)).astype(bf16)
    residual = contract(own, 1, came[:, 1].reshape(256, 128), 1)
    second = exchange_far(mixed, Z, FIRST_LAST).astype(f32).sum(axis=0)
    second = (second + residual).astype(bf16)

    kept = jnp.stack(
        [state_first, state_second, branch_first.astype(f32), branch_second.astype(f32)]
    )
    kept = kept.reshape(4, 8, 4, 32).transpose(2, 0, 1, 3).reshape(4, 8, 128)
    kept = jnp.stack(in_order(traded(kept, "y"), "y"))
    kept = kept.reshape(4, 4, 8, 32).transpose(1, 0, 2, 3).reshape(2, LAYERS, 32, 32)
    living = lengths[:, None, None] >= depth - jnp.arange(2, dtype=jnp.int32)[:, None]
    history = jnp.where(living, prior_window[:, :, 1:], jnp.zeros_like(prior_window[:, :, 1:]))
    window = jnp.concatenate([history, kept[1].astype(bf16)[:, :, None]], axis=2)
    return second.T, kept[0], window


def solution(mesh):
    torus = Mesh(mesh.devices.reshape(8, 2, 2, 4, 4, 2), AXES)
    in_specs = (
        P(None, DP + TP),
        P(DP),
        P(None, DP, TP),
        P(None, DP, None, TP),
        P(None, DP),
        P(None, DP, TP),
        P(None, DP, TP),
        P(None, None, TP),
        P(None, None, TP),
        P(None, None, TP),
        P(None, TP),
        P(None, TP, DP),
    )
    out_specs = (P(None, DP + TP), P(None, DP, TP), P(None, DP, None, TP))
    return jax.shard_map(
        both_blocks, mesh=torus, in_specs=in_specs, out_specs=out_specs, check_vma=False
    )
```

```python
import jax
import jax.numpy as jnp
from jax import lax
from jax.experimental import pallas as pl
from jax.experimental.pallas import tpu as pltpu
from jax.sharding import Mesh
from jax.sharding import PartitionSpec as P


D = 4096
BLOCK = 256
LAYERS = 2
TAPS = 4
AXES = ("zh", "zm", "zl", "y", "x", "core")
Z = ("zh", "zm", "zl")
ZQ = ("zm", "zl")
TP = ("zh", "zm", "zl", "y")
DP = ("x", "core")
PLANE = ("x", "core", "y")
PAIRED_PLANE = ("zl", "y", "x", "core")
FIRST_GATHER = 22
FIRST_REDUCE = 3
FIRST_LAST = 18
bf16 = jnp.bfloat16
f32 = jnp.float32


epsilon = 1e-06


def exchange(tiles, axes):
    return lax.all_to_all(tiles, axes, 0, 0, tiled=True)


def exchange_far(tiles, axes, first):
    count = lax.axis_size(axes)
    order = [(first + at) % count for at in range(count)]
    return lax.all_to_all(tiles, axes, 0, 0, axis_index_groups=[order], tiled=True)


def everywhere(array, axes, first):
    count = lax.axis_size(axes)
    tiles = jnp.broadcast_to(array[None], (count, *array.shape))
    return exchange_far(tiles, axes, first)


def passed(piece, axis, flip):
    return lax.ppermute(piece, axis, [(at, at ^ flip) for at in range(lax.axis_size(axis))])


def traded(tiles, axis):
    here = lax.axis_index(axis)
    tiles = tiles if isinstance(tiles, list) else [tiles] * 4
    pieces = [lax.dynamic_slice_in_dim(tiles[flip], here ^ flip, 1)[0] for flip in range(4)]
    return pieces[:1] + [passed(pieces[flip], axis, flip) for flip in range(1, 4)]


def in_order(pieces, axis):
    here = lax.axis_index(axis)
    pieces = [jnp.where((here & 1) == 1, pieces[k ^ 1], pieces[k]) for k in range(4)]
    return [jnp.where(here > 1, pieces[k ^ 2], pieces[k]) for k in range(4)]


def whole_of(coarse, middle, fine):
    return coarse.astype(f32) + (middle.astype(f32) + fine.astype(f32))


def contract(a, a_dim, b, b_dim):
    return lax.dot_general(a, b, (((a_dim,), (b_dim,)), ((), ())), preferred_element_type=f32)


def grouped_features(rows_by_feature, first):
    width = rows_by_feature.shape[1]
    to = jnp.arange(width, dtype=jnp.int32)
    source = ((to % 128) // 4 + first) % 32 * 16 + to // 128 * 4 + to % 4
    chosen = (jnp.arange(width, dtype=jnp.int32)[:, None] == source[None, :]).astype(bf16)
    return contract(rows_by_feature, 1, chosen, 0).astype(bf16)


def pack_kernel(branch, gate, out, in_gate, rec_gate, gain, state, window, taps, decay, packed, later):
    row = lax.broadcasted_iota(jnp.int32, (8, 32), 0)
    weights = [
        (weight[layer].astype(f32) * gain[layer : layer + 1]).astype(bf16)
        for layer in range(2)
        for weight in (branch, gate)
    ]
    width = 512
    to = lax.broadcasted_iota(jnp.int32, (width, width), 1)
    source = (((to & 127) >> 2) + FIRST_GATHER & 31) * 16 + (to >> 7) * 4 + (to & 3)
    chosen = lax.broadcasted_iota(jnp.int32, (width, width), 0) == source
    chosen = jnp.where(chosen, 1.0, 0.0).astype(bf16)
    weights = jnp.concatenate([*weights, out[0]], axis=0)
    weights = jnp.dot(weights, chosen, preferred_element_type=f32).astype(bf16)

    def split(value):
        coarse = value.astype(bf16).astype(f32)
        middle = (value - coarse).astype(bf16).astype(f32)
        return [coarse, middle, value - coarse - middle]

    rates = split(jnp.where((row & 1) == 0, decay[:1], decay[1:2]))
    rates = jnp.where(row < 2, rates[0], jnp.where(row < 4, rates[1], rates[2]))
    rates = jnp.where(row < 6, rates, 0.0)
    tap_rows = jnp.concatenate([taps[0].astype(f32), taps[1].astype(f32)], axis=0)
    none = jnp.zeros((32, 32), f32)
    small = [part for layer in range(2) for part in split(state[layer])]
    small = small + [jnp.concatenate([rates] * 4, axis=0), none]
    small = small + [window[layer, tap].astype(f32) for layer in range(2) for tap in range(3)]
    small = small + [jnp.concatenate([tap_rows] * 4, axis=0), none]
    small = [jnp.concatenate(small[4 * at : 4 * at + 4], axis=1) for at in range(4)]
    for y in range(4):
        packed[y, :64] = weights[:64, 128 * y : 128 * (y + 1)]
        for kind, weight in enumerate((in_gate, rec_gate)):
            for half in range(2):
                place = 64 + 32 * (2 * kind + half)
                packed[y, place : place + 32] = weight[0, :, 128 * half : 128 * (half + 1)]
        for q in range(4):
            place = 192 + 32 * q
            packed[y, place : place + 32] = weights[128:, 128 * q : 128 * (q + 1)]
        later[y] = weights[64:128, 128 * y : 128 * (y + 1)]
        for at in range(4):
            place = 320 + 8 * at
            packed[y, place : place + 8] = small[at][8 * y : 8 * (y + 1)].astype(bf16)


def packed_for_y(*arrays):
    return pl.pallas_call(
        pack_kernel,
        out_shape=[
            jax.ShapeDtypeStruct((4, 352, 128), bf16),
            jax.ShapeDtypeStruct((4, 64, 128), bf16),
        ],
        compiler_params=pltpu.CompilerParams(vmem_limit_bytes=8 * 2**20),
        cost_estimate=pl.CostEstimate(flops=100_000_000, bytes_accessed=800_000, transcendentals=0),
    )(*arrays)


def gated_step(branch, gate_in, upper, history, taps, gates, decay, earlier):
    convolved = (
        jnp.sum(history * taps[:3, None], axis=0) + branch.astype(f32) * taps[3]
    ).astype(bf16)
    half = BLOCK // 2
    mapped = jax.nn.sigmoid(contract(convolved, 1, gates, 1))
    input_gate, recur_gate = mapped[:, :half], mapped[:, half:]
    own = jnp.where(upper, convolved[:, half:], convolved[:, :half])
    log_keep = 8.0 * recur_gate * decay
    keeping = jnp.exp(log_keep)
    feeding = jnp.sqrt(-jnp.expm1(2.0 * log_keep))
    state = keeping * earlier + feeding * input_gate * own.astype(f32)
    readout = (state * jax.nn.gelu(gate_in.astype(f32))).astype(bf16)
    own_branch = jnp.where(upper, branch[:, half:], branch[:, :half])
    return state, own_branch, readout


def both_blocks(
    stream,
    lengths,
    prior_state,
    prior_window,
    norm_gain,
    w_branch,
    w_gate_branch,
    conv_taps,
    w_in_gate,
    w_rec_gate,
    decay_param,
    w_out,
):
    zl = lax.axis_index("zl")
    upper = zl == 1

    stream_t = everywhere(stream.T, Z, FIRST_GATHER).reshape(128, 256)

    second_gate_rows = jnp.concatenate(
        [
            weight[1, 128 * half : 128 * (half + 1)].T
            for weight in (w_in_gate, w_rec_gate)
            for half in range(2)
        ]
    )
    depth = TAPS - 1

    def for_each(rows):
        return jnp.broadcast_to(rows.reshape(1, -1, 128), (4, rows.size // 128, 128))

    near, second_weights = packed_for_y(
        w_branch.transpose(0, 2, 1),
        w_gate_branch.transpose(0, 2, 1),
        w_out,
        w_in_gate.transpose(0, 2, 1),
        w_rec_gate.transpose(0, 2, 1),
        norm_gain,
        prior_state,
        prior_window.transpose(0, 2, 1, 3),
        conv_taps,
        decay_param,
    )
    near = jnp.stack(in_order(traded(near, "y"), "y"))
    w_first = near[:, :64].reshape(4, 2, 32, 128).transpose(1, 0, 2, 3).reshape(2, 128, 128)
    index = lax.broadcasted_iota(jnp.int32, (128, 128), 0)
    same = (index == lax.broadcasted_iota(jnp.int32, (128, 128), 1)).astype(bf16)
    w_first = jnp.concatenate(
        [w_first[0], jnp.where(upper, same, w_first[1]), jnp.where(upper, w_first[1], same)]
    )

    def gates_of(rows):
        rows = rows.reshape(4, 2, 2, 32, 128).transpose(1, 0, 3, 2, 4)
        return rows.reshape(256, 256)

    gates = gates_of(near[:, 64:192])

    def by_group(rows):
        rows = rows.reshape(4, -1, 8, 4, 32).transpose(1, 3, 2, 0, 4)
        return rows.reshape(-1, 8, 128)

    groups = by_group(near[:, 320:])
    shared = jnp.concatenate(
        [
            near[:, 192:320].reshape(4, 4, 32, 128).transpose(1, 0, 2, 3).reshape(4, 128, 128),
            second_weights,
        ],
        axis=1,
    )
    with_windows = jnp.concatenate([shared, for_each(near[:, 336:])], axis=1)
    shared = traded([shared, with_windows, shared, shared], ZQ)
    partner = by_group(shared[1][192:].reshape(4, 16, 128))
    windows = jnp.concatenate(
        [jnp.where(upper, partner, groups[8:]), jnp.where(upper, groups[8:], partner)], axis=2
    ).astype(f32)
    shared = in_order([piece[:192] for piece in shared], ZQ)
    w_mid = jnp.concatenate([piece[:128] for piece in shared])
    later_rows = jnp.concatenate(
        [
            for_each(second_gate_rows),
            for_each(jnp.concatenate([piece[128:] for piece in shared])),
            grouped_features(w_out[1], FIRST_LAST).reshape(32, 4, 128).transpose(1, 0, 2),
        ],
        axis=1,
    )
    later_rows = jnp.stack(in_order(traded(later_rows, "y"), "y"))
    gates_second = gates_of(later_rows[:, :128])
    w_second = (
        later_rows[:, 128:384]
        .reshape(4, 4, 2, 32, 128)
        .transpose(1, 2, 0, 3, 4)
        .reshape(1024, 128)
    )
    w_last = later_rows[:, 384:].reshape(128, 128)

    own_lengths = lax.dynamic_slice_in_dim(lengths, lax.axis_index("y") * 8, 8)[:, None]
    earlier_rows = [
        jnp.where(own_lengths >= 2, whole_of(*groups[3 * layer : 3 * layer + 3]), 0.0)
        for layer in range(LAYERS)
    ]
    decay = whole_of(groups[6][:2], groups[6][2:4], groups[6][4:6])[:, None]
    decay = jax.nn.log_sigmoid(decay)
    needed = depth + 1 - jnp.arange(depth, dtype=jnp.int32)
    history_rows = jnp.where(
        own_lengths >= needed[:, None, None], windows[:6].reshape(LAYERS, depth, 8, 256), 0.0
    )
    taps = windows[6].reshape(LAYERS, TAPS, 256)

    products = contract(stream_t, 0, w_first, 1).astype(bf16)
    products = products.reshape(8, 4, 8, 3, 128).transpose(3, 1, 0, 2, 4)
    sent = jnp.stack(
        [
            jnp.stack([products[0], products[1]], axis=2),
            jnp.stack([products[0], products[2]], axis=2),
        ]
    )
    came = exchange(sent.reshape(64, 16, 128), PAIRED_PLANE)
    came = came.reshape(2, 32, 2, 8, 128)
    later = (history_rows[1], taps[1], decay[1], earlier_rows[1])
    branch = came[:, :, 0].astype(f32).sum(axis=1)
    branch = jnp.concatenate([branch[0], branch[1]], axis=1)
    rows = jnp.where(upper, came[0, :, 1], came[1, :, 1])
    gate_in = jnp.where(upper, came[1, :, 1], came[0, :, 1]).astype(f32).sum(axis=0)
    widened = rows.astype(f32)
    squares = jnp.sum(jnp.sum(widened * widened, axis=0), axis=1, keepdims=True)
    scaling = lax.rsqrt(squares / D + epsilon)
    state_first, branch_first, readout = gated_step(
        (branch * scaling).astype(bf16),
        (gate_in * scaling).astype(bf16),
        upper,
        history_rows[0],
        taps[0],
        gates,
        decay[0],
        earlier_rows[0],
    )
    sent = jnp.stack([jnp.broadcast_to(readout[None], (32, 8, 128)), rows], axis=1)
    came = exchange(sent.reshape(32, 16, 128), ZQ + DP).reshape(4, 8, 2, 8, 128)
    residual = came[0, :, 1].reshape(64, 128).astype(f32)
    came = came[:, :, 0].reshape(4, 64, 128)
    came = jnp.concatenate([came[at] for at in range(4)], axis=1)
    mixed = contract(came, 1, w_mid, 0).astype(bf16)
    mixed = everywhere(mixed, "zh", FIRST_REDUCE)
    at_z = lax.axis_index(Z)
    mixed, w_second, gates_second, w_last, state_first, branch_first, at_z = (
        lax.optimization_barrier(
            (mixed, w_second, gates_second, w_last, state_first, branch_first, at_z)
        )
    )
    mixed = mixed.astype(f32).sum(axis=0)
    first = (mixed + residual).astype(bf16)

    products = contract(first, 1, w_second, 1).astype(bf16)
    products = [products[:, 128 * at : 128 * (at + 1)].reshape(8, 8, 128) for at in range(8)]
    own_rows = first.reshape(8, 8, 128)
    sent = jnp.stack(
        [
            jnp.stack(
                [
                    products[4 * zm],
                    products[4 * zm + 2],
                    products[4 * zm + 2 * low + 1],
                    own_rows,
                ],
                axis=1,
            )
            for zm in range(2)
            for low in range(2)
        ]
    )
    came = exchange(sent.reshape(32, 32, 128), ZQ + DP).reshape(32, 4, 8, 128)
    came, state_first, branch_first = lax.optimization_barrier((came, state_first, branch_first))
    rows = came[:, 3]
    came = came[:, :3].astype(f32).sum(axis=0)
    widened = rows.astype(f32)
    squares = jnp.sum(jnp.sum(widened * widened, axis=0), axis=1, keepdims=True)
    branch = jnp.concatenate([came[0], came[1]], axis=1)
    scaling = lax.rsqrt(squares / D + epsilon)
    state_second, branch_second, readout = gated_step(
        (branch * scaling).astype(bf16),
        (came[2] * scaling).astype(bf16),
        upper,
        later[0],
        later[1],
        gates_second,
        later[2],
        later[3],
    )
    sent = jnp.stack(
        [
            jnp.broadcast_to(readout[None], (32, 8, 128)),
            rows.reshape(4, 8, 8, 128).transpose(1, 0, 2, 3).reshape(32, 8, 128),
        ],
        axis=1,
    )
    came = exchange(sent.reshape(32, 16, 128), PLANE).reshape(32, 2, 8, 128)
    came, lengths, prior_window, at_z = lax.optimization_barrier(
        (came, lengths, prior_window, at_z)
    )
    mixed = contract(w_last, 0, came[:, 0].reshape(256, 128), 1).astype(bf16)
    mixed = mixed.reshape(32, 4, 256)
    own = (at_z + (32 - FIRST_GATHER) & 31) * 4
    own = lax.broadcasted_iota(jnp.int32, (4, 128), 0) + own
    own = (own == lax.broadcasted_iota(jnp.int32, (4, 128), 1)).astype(bf16)
    residual = contract(own, 1, came[:, 1].reshape(256, 128), 1)
    second = exchange_far(mixed, Z, FIRST_LAST).astype(f32).sum(axis=0)
    second = (second + residual).astype(bf16)

    kept = jnp.stack(
        [state_first, state_second, branch_first.astype(f32), branch_second.astype(f32)]
    )
    kept = kept.reshape(4, 8, 4, 32).transpose(2, 0, 1, 3).reshape(4, 8, 128)
    kept = jnp.stack(in_order(traded(kept, "y"), "y"))
    kept = kept.reshape(4, 4, 8, 32).transpose(1, 0, 2, 3).reshape(2, LAYERS, 32, 32)
    living = lengths[:, None, None] >= depth - jnp.arange(2, dtype=jnp.int32)[:, None]
    history = jnp.where(living, prior_window[:, :, 1:], jnp.zeros_like(prior_window[:, :, 1:]))
    window = jnp.concatenate([history, kept[1].astype(bf16)[:, :, None]], axis=2)
    return second.T, kept[0], window


def solution(mesh):
    torus = Mesh(mesh.devices.reshape(8, 2, 2, 4, 4, 2), AXES)
    in_specs = (
        P(None, DP + TP),
        P(DP),
        P(None, DP, TP),
        P(None, DP, None, TP),
        P(None, DP),
        P(None, DP, TP),
        P(None, DP, TP),
        P(None, None, TP),
        P(None, None, TP),
        P(None, None, TP),
        P(None, TP),
        P(None, TP, DP),
    )
    out_specs = (P(None, DP + TP), P(None, DP, TP), P(None, DP, None, TP))
    return jax.shard_map(
        both_blocks, mesh=torus, in_specs=in_specs, out_specs=out_specs, check_vma=False
    )
```

```python
import jax
import jax.numpy as jnp
from jax import lax
from jax.experimental import pallas as pl
from jax.experimental.pallas import tpu as pltpu
from jax.sharding import Mesh
from jax.sharding import PartitionSpec as P


D = 4096
BLOCK = 256
LAYERS = 2
TAPS = 4
AXES = ("zh", "zm", "zl", "y", "x", "core")
Z = ("zh", "zm", "zl")
ZQ = ("zm", "zl")
TP = ("zh", "zm", "zl", "y")
DP = ("x", "core")
PLANE = ("x", "core", "y")
PAIRED_PLANE = ("zl", "y", "x", "core")
FIRST_GATHER = 22
FIRST_REDUCE = 4
FIRST_LAST = 18
bf16 = jnp.bfloat16
f32 = jnp.float32


epsilon = 1e-06


def exchange(tiles, axes):
    return lax.all_to_all(tiles, axes, 0, 0, tiled=True)


def exchange_far(tiles, axes, first):
    count = lax.axis_size(axes)
    order = [(first + at) % count for at in range(count)]
    return lax.all_to_all(tiles, axes, 0, 0, axis_index_groups=[order], tiled=True)


def everywhere(array, axes, first):
    count = lax.axis_size(axes)
    tiles = jnp.broadcast_to(array[None], (count, *array.shape))
    return exchange_far(tiles, axes, first)


def passed(piece, axis, flip):
    return lax.ppermute(piece, axis, [(at, at ^ flip) for at in range(lax.axis_size(axis))])


def traded(tiles, axis):
    here = lax.axis_index(axis)
    tiles = tiles if isinstance(tiles, list) else [tiles] * 4
    pieces = [lax.dynamic_slice_in_dim(tiles[flip], here ^ flip, 1)[0] for flip in range(4)]
    return pieces[:1] + [passed(pieces[flip], axis, flip) for flip in range(1, 4)]


def in_order(pieces, axis):
    here = lax.axis_index(axis)
    pieces = [jnp.where((here & 1) == 1, pieces[k ^ 1], pieces[k]) for k in range(4)]
    return [jnp.where(here > 1, pieces[k ^ 2], pieces[k]) for k in range(4)]


def whole_of(coarse, middle, fine):
    return coarse.astype(f32) + (middle.astype(f32) + fine.astype(f32))


def contract(a, a_dim, b, b_dim):
    return lax.dot_general(a, b, (((a_dim,), (b_dim,)), ((), ())), preferred_element_type=f32)


def grouped_features(rows_by_feature, first):
    width = rows_by_feature.shape[1]
    to = jnp.arange(width, dtype=jnp.int32)
    source = ((to % 128) // 4 + first) % 32 * 16 + to // 128 * 4 + to % 4
    chosen = (jnp.arange(width, dtype=jnp.int32)[:, None] == source[None, :]).astype(bf16)
    return contract(rows_by_feature, 1, chosen, 0).astype(bf16)


def pack_kernel(branch, gate, out, in_gate, rec_gate, gain, state, window, taps, decay, packed, later):
    row = lax.broadcasted_iota(jnp.int32, (8, 32), 0)
    weights = [
        (weight[layer].astype(f32) * gain[layer : layer + 1]).astype(bf16)
        for layer in range(2)
        for weight in (branch, gate)
    ]
    width = 512
    to = lax.broadcasted_iota(jnp.int32, (width, width), 1)
    source = (((to & 127) >> 2) + FIRST_GATHER & 31) * 16 + (to >> 7) * 4 + (to & 3)
    chosen = lax.broadcasted_iota(jnp.int32, (width, width), 0) == source
    chosen = jnp.where(chosen, 1.0, 0.0).astype(bf16)
    weights = jnp.concatenate([*weights, out[0]], axis=0)
    weights = jnp.dot(weights, chosen, preferred_element_type=f32).astype(bf16)

    def split(value):
        coarse = value.astype(bf16).astype(f32)
        middle = (value - coarse).astype(bf16).astype(f32)
        return [coarse, middle, value - coarse - middle]

    rates = split(jnp.where((row & 1) == 0, decay[:1], decay[1:2]))
    rates = jnp.where(row < 2, rates[0], jnp.where(row < 4, rates[1], rates[2]))
    rates = jnp.where(row < 6, rates, 0.0)
    tap_rows = jnp.concatenate([taps[0].astype(f32), taps[1].astype(f32)], axis=0)
    none = jnp.zeros((32, 32), f32)
    small = [part for layer in range(2) for part in split(state[layer])]
    small = small + [jnp.concatenate([rates] * 4, axis=0), none]
    small = small + [window[layer, tap].astype(f32) for layer in range(2) for tap in range(3)]
    small = small + [jnp.concatenate([tap_rows] * 4, axis=0), none]
    small = [jnp.concatenate(small[4 * at : 4 * at + 4], axis=1) for at in range(4)]
    for y in range(4):
        packed[y, :64] = weights[:64, 128 * y : 128 * (y + 1)]
        for kind, weight in enumerate((in_gate, rec_gate)):
            for half in range(2):
                place = 64 + 32 * (2 * kind + half)
                packed[y, place : place + 32] = weight[0, :, 128 * half : 128 * (half + 1)]
        for q in range(4):
            place = 192 + 32 * q
            packed[y, place : place + 32] = weights[128:, 128 * q : 128 * (q + 1)]
        later[y] = weights[64:128, 128 * y : 128 * (y + 1)]
        for at in range(4):
            place = 320 + 8 * at
            packed[y, place : place + 8] = small[at][8 * y : 8 * (y + 1)].astype(bf16)


def packed_for_y(*arrays):
    return pl.pallas_call(
        pack_kernel,
        out_shape=[
            jax.ShapeDtypeStruct((4, 352, 128), bf16),
            jax.ShapeDtypeStruct((4, 64, 128), bf16),
        ],
        compiler_params=pltpu.CompilerParams(vmem_limit_bytes=8 * 2**20),
        cost_estimate=pl.CostEstimate(flops=100_000_000, bytes_accessed=800_000, transcendentals=0),
    )(*arrays)


def gated_step(branch, gate_in, upper, history, taps, gates, decay, earlier):
    convolved = (
        jnp.sum(history * taps[:3, None], axis=0) + branch.astype(f32) * taps[3]
    ).astype(bf16)
    half = BLOCK // 2
    mapped = jax.nn.sigmoid(contract(convolved, 1, gates, 1))
    input_gate, recur_gate = mapped[:, :half], mapped[:, half:]
    own = jnp.where(upper, convolved[:, half:], convolved[:, :half])
    log_keep = 8.0 * recur_gate * decay
    keeping = jnp.exp(log_keep)
    feeding = jnp.sqrt(-jnp.expm1(2.0 * log_keep))
    state = keeping * earlier + feeding * input_gate * own.astype(f32)
    readout = (state * jax.nn.gelu(gate_in.astype(f32))).astype(bf16)
    own_branch = jnp.where(upper, branch[:, half:], branch[:, :half])
    return state, own_branch, readout


def both_blocks(
    stream,
    lengths,
    prior_state,
    prior_window,
    norm_gain,
    w_branch,
    w_gate_branch,
    conv_taps,
    w_in_gate,
    w_rec_gate,
    decay_param,
    w_out,
):
    zl = lax.axis_index("zl")
    upper = zl == 1

    stream_t = everywhere(stream.T, Z, FIRST_GATHER).reshape(128, 256)

    second_gate_rows = jnp.concatenate(
        [
            weight[1, 128 * half : 128 * (half + 1)].T
            for weight in (w_in_gate, w_rec_gate)
            for half in range(2)
        ]
    )
    depth = TAPS - 1

    def for_each(rows):
        return jnp.broadcast_to(rows.reshape(1, -1, 128), (4, rows.size // 128, 128))

    near, second_weights = packed_for_y(
        w_branch.transpose(0, 2, 1),
        w_gate_branch.transpose(0, 2, 1),
        w_out[:1],
        w_in_gate[:1].transpose(0, 2, 1),
        w_rec_gate[:1].transpose(0, 2, 1),
        norm_gain,
        prior_state,
        prior_window.transpose(0, 2, 1, 3),
        conv_taps,
        decay_param,
    )
    near = jnp.stack(in_order(traded(near, "y"), "y"))
    w_first = near[:, :64].reshape(4, 2, 32, 128).transpose(1, 0, 2, 3).reshape(2, 128, 128)
    index = lax.broadcasted_iota(jnp.int32, (128, 128), 0)
    same = (index == lax.broadcasted_iota(jnp.int32, (128, 128), 1)).astype(bf16)
    w_first = jnp.concatenate(
        [w_first[0], jnp.where(upper, same, w_first[1]), jnp.where(upper, w_first[1], same)]
    )

    def gates_of(rows):
        rows = rows.reshape(4, 2, 2, 32, 128).transpose(1, 0, 3, 2, 4)
        return rows.reshape(256, 256)

    gates = gates_of(near[:, 64:192])

    def by_group(rows):
        rows = rows.reshape(4, -1, 8, 4, 32).transpose(1, 3, 2, 0, 4)
        return rows.reshape(-1, 8, 128)

    groups = by_group(near[:, 320:])
    shared = jnp.concatenate(
        [
            near[:, 192:320].reshape(4, 4, 32, 128).transpose(1, 0, 2, 3).reshape(4, 128, 128),
            second_weights,
        ],
        axis=1,
    )
    with_windows = jnp.concatenate([shared, for_each(near[:, 336:])], axis=1)
    shared = traded([shared, with_windows, shared, shared], ZQ)
    partner = by_group(shared[1][192:].reshape(4, 16, 128))
    windows = jnp.concatenate(
        [jnp.where(upper, partner, groups[8:]), jnp.where(upper, groups[8:], partner)], axis=2
    ).astype(f32)
    shared = in_order([piece[:192] for piece in shared], ZQ)
    w_mid = jnp.concatenate([piece[:128] for piece in shared])
    later_rows = jnp.concatenate(
        [
            for_each(second_gate_rows),
            for_each(jnp.concatenate([piece[128:] for piece in shared])),
            grouped_features(w_out[1], FIRST_LAST).reshape(32, 4, 128).transpose(1, 0, 2),
        ],
        axis=1,
    )
    later_rows = jnp.stack(in_order(traded(later_rows, "y"), "y"))
    gates_second = gates_of(later_rows[:, :128])
    w_second = (
        later_rows[:, 128:384]
        .reshape(4, 4, 2, 32, 128)
        .transpose(1, 2, 0, 3, 4)
        .reshape(1024, 128)
    )
    w_last = later_rows[:, 384:].reshape(128, 128)

    own_lengths = lax.dynamic_slice_in_dim(lengths, lax.axis_index("y") * 8, 8)[:, None]
    earlier_rows = [
        jnp.where(own_lengths >= 2, whole_of(*groups[3 * layer : 3 * layer + 3]), 0.0)
        for layer in range(LAYERS)
    ]
    decay = whole_of(groups[6][:2], groups[6][2:4], groups[6][4:6])[:, None]
    decay = jax.nn.log_sigmoid(decay)
    needed = depth + 1 - jnp.arange(depth, dtype=jnp.int32)
    history_rows = jnp.where(
        own_lengths >= needed[:, None, None], windows[:6].reshape(LAYERS, depth, 8, 256), 0.0
    )
    taps = windows[6].reshape(LAYERS, TAPS, 256)

    products = contract(stream_t, 0, w_first, 1).astype(bf16)
    products = products.reshape(8, 4, 8, 3, 128).transpose(3, 1, 0, 2, 4)
    sent = jnp.stack(
        [
            jnp.stack([products[0], products[1]], axis=2),
            jnp.stack([products[0], products[2]], axis=2),
        ]
    )
    came = exchange(sent.reshape(64, 16, 128), PAIRED_PLANE)
    came = came.reshape(2, 32, 2, 8, 128)
    later = (history_rows[1], taps[1], decay[1], earlier_rows[1])
    branch = came[:, :, 0].astype(f32).sum(axis=1)
    branch = jnp.concatenate([branch[0], branch[1]], axis=1)
    rows = jnp.where(upper, came[0, :, 1], came[1, :, 1])
    gate_in = jnp.where(upper, came[1, :, 1], came[0, :, 1]).astype(f32).sum(axis=0)
    widened = rows.astype(f32)
    squares = jnp.sum(jnp.sum(widened * widened, axis=0), axis=1, keepdims=True)
    scaling = lax.rsqrt(squares / D + epsilon)
    state_first, branch_first, readout = gated_step(
        (branch * scaling).astype(bf16),
        (gate_in * scaling).astype(bf16),
        upper,
        history_rows[0],
        taps[0],
        gates,
        decay[0],
        earlier_rows[0],
    )
    sent = jnp.stack([jnp.broadcast_to(readout[None], (32, 8, 128)), rows], axis=1)
    came = exchange(sent.reshape(32, 16, 128), ZQ + DP).reshape(4, 8, 2, 8, 128)
    residual = came[0, :, 1].reshape(64, 128).astype(f32)
    came = came[:, :, 0].reshape(4, 64, 128)
    came = jnp.concatenate([came[at] for at in range(4)], axis=1)
    mixed = contract(came, 1, w_mid, 0).astype(bf16)
    mixed = everywhere(mixed, "zh", FIRST_REDUCE)
    at_z = lax.axis_index(Z)
    mixed, w_second, gates_second, w_last, state_first, branch_first, at_z = (
        lax.optimization_barrier(
            (mixed, w_second, gates_second, w_last, state_first, branch_first, at_z)
        )
    )
    mixed = mixed.astype(f32).sum(axis=0)
    first = (mixed + residual).astype(bf16)

    products = contract(first, 1, w_second, 1).astype(bf16)
    products = [products[:, 128 * at : 128 * (at + 1)].reshape(8, 8, 128) for at in range(8)]
    own_rows = first.reshape(8, 8, 128)
    sent = jnp.stack(
        [
            jnp.stack(
                [
                    products[4 * zm],
                    products[4 * zm + 2],
                    products[4 * zm + 2 * low + 1],
                    own_rows,
                ],
                axis=1,
            )
            for zm in range(2)
            for low in range(2)
        ]
    )
    came = exchange(sent.reshape(32, 32, 128), ZQ + DP).reshape(32, 4, 8, 128)
    came, state_first, branch_first = lax.optimization_barrier((came, state_first, branch_first))
    rows = came[:, 3]
    came = came[:, :3].astype(f32).sum(axis=0)
    widened = rows.astype(f32)
    squares = jnp.sum(jnp.sum(widened * widened, axis=0), axis=1, keepdims=True)
    branch = jnp.concatenate([came[0], came[1]], axis=1)
    scaling = lax.rsqrt(squares / D + epsilon)
    state_second, branch_second, readout = gated_step(
        (branch * scaling).astype(bf16),
        (came[2] * scaling).astype(bf16),
        upper,
        later[0],
        later[1],
        gates_second,
        later[2],
        later[3],
    )
    sent = jnp.stack(
        [
            jnp.broadcast_to(readout[None], (32, 8, 128)),
            rows.reshape(4, 8, 8, 128).transpose(1, 0, 2, 3).reshape(32, 8, 128),
        ],
        axis=1,
    )
    came = exchange(sent.reshape(32, 16, 128), PLANE).reshape(32, 2, 8, 128)
    came, lengths, prior_window, at_z = lax.optimization_barrier(
        (came, lengths, prior_window, at_z)
    )
    mixed = contract(w_last, 0, came[:, 0].reshape(256, 128), 1).astype(bf16)
    mixed = mixed.reshape(32, 4, 256)
    own = (at_z + (32 - FIRST_GATHER) & 31) * 4
    own = lax.broadcasted_iota(jnp.int32, (4, 128), 0) + own
    own = (own == lax.broadcasted_iota(jnp.int32, (4, 128), 1)).astype(bf16)
    residual = contract(own, 1, came[:, 1].reshape(256, 128), 1)
    second = exchange_far(mixed, Z, FIRST_LAST).astype(f32).sum(axis=0)
    second = (second + residual).astype(bf16)

    kept = jnp.stack(
        [state_first, state_second, branch_first.astype(f32), branch_second.astype(f32)]
    )
    kept = kept.reshape(4, 8, 4, 32).transpose(2, 0, 1, 3).reshape(4, 8, 128)
    kept = jnp.stack(in_order(traded(kept, "y"), "y"))
    kept = kept.reshape(4, 4, 8, 32).transpose(1, 0, 2, 3).reshape(2, LAYERS, 32, 32)
    living = lengths[:, None, None] >= depth - jnp.arange(2, dtype=jnp.int32)[:, None]
    history = jnp.where(living, prior_window[:, :, 1:], jnp.zeros_like(prior_window[:, :, 1:]))
    window = jnp.concatenate([history, kept[1].astype(bf16)[:, :, None]], axis=2)
    return second.T, kept[0], window


def solution(mesh):
    torus = Mesh(mesh.devices.reshape(8, 2, 2, 4, 4, 2), AXES)
    in_specs = (
        P(None, DP + TP),
        P(DP),
        P(None, DP, TP),
        P(None, DP, None, TP),
        P(None, DP),
        P(None, DP, TP),
        P(None, DP, TP),
        P(None, None, TP),
        P(None, None, TP),
        P(None, None, TP),
        P(None, TP),
        P(None, TP, DP),
    )
    out_specs = (P(None, DP + TP), P(None, DP, TP), P(None, DP, None, TP))
    return jax.shard_map(
        both_blocks, mesh=torus, in_specs=in_specs, out_specs=out_specs, check_vma=False
    )
```
